256 devices in a mesh: ra: 32 (over z, y), cb: 8 (over x, core).
Axes of the slice: x: 4, y: 4, z: 8, core: 2. Of those that a mesh axis runs over, the one named last changes fastest.
Arguments:
- stream: bfloat16 [64, 1024], P(None, 'ra'), may hold values from -24 to 24, as said below
- gain_first: float32 [1024], P('ra'), may hold values from 0.5 to 1.5
- up_first: float32 [1024, 4096], P('ra', 'cb'), may hold values from -0.1875 to 0.1875
- down_first: float32 [4096, 1024], P('cb', 'ra'), may hold values from -0.09375 to 0.09375
- gain_second: float32 [1024], P('ra'), may hold values from 0.5 to 1.5
- up_second: float32 [1024, 4096], P('ra', 'cb'), may hold values from -0.1875 to 0.1875
- down_second: float32 [4096, 1024], P('cb', 'ra'), may hold values from -0.09375 to 0.09375
Outputs:
- read: bfloat16 [64, 1024], P(None, 'ra')
The draws below stay inside these ranges and needn't reach their ends.
Inputs may be any that keep to these rules, and one draw needn't show every extreme that they name: stream is of order one, and in each token one aligned block of 32 features is four times larger than the rest.
All inputs are finite; a program needn't handle non-finite values.
Results may differ from the reference program's by a relative error of at most 0.025.
Values may be sent and summed in bfloat16 or wider, within the bound.
A program may use at most 64 MiB of HBM per device.

```python
import jax
import jax.numpy as jnp
from jax import lax

D = 1024
FF = 4096
TOKENS = 64
COLS_RA = 32


def draw_stream(key, part):
    key_base, key_block = jax.random.split(key)
    base = jnp.clip(jax.random.normal(key_base, (TOKENS, D), jnp.float32), -6.0, 6.0)
    chosen = jax.random.randint(key_block, (TOKENS, 1), 0, D // COLS_RA)
    column_block = jnp.arange(D, dtype=jnp.int32)[None, :] // COLS_RA
    boosted = jnp.where(column_block == chosen, 4.0, 1.0)
    return (base * boosted).astype(jnp.bfloat16)


def shard_levels(rng, shape, cuts, low, largest):
    level, own = 1.0, jax.random.fold_in(rng, 6)
    for axis_at, shards_of in cuts:
        draws = jnp.exp(jax.random.uniform(jax.random.fold_in(own, axis_at), (shards_of,), jnp.float32, low / len(cuts), largest / len(cuts)))
        level = level * jnp.repeat(draws, shape[axis_at] // shards_of).reshape([-1 if axis == axis_at else 1 for axis in range(len(shape))])
    return level


def normal_values(own_key, extent, width, most, shards=(), held_as=jnp.bfloat16):
    gain = shard_levels(own_key, extent, shards, -0.22, 0.18) if shards else 1.0
    result = jax.random.normal(own_key, extent, jnp.float32) * width * gain
    return jnp.minimum(jnp.maximum(result, -most), most).astype(held_as)


def setup_inputs(seed: int = 0) -> dict:
    arg_keys = jax.random.split(jax.random.key(seed), 8)
    return {
        "stream": draw_stream(jax.random.fold_in(arg_keys[7], 71), 0),
        "gain_first": jnp.clip(1.0 + 0.1 * jax.random.normal(arg_keys[1], (D,), jnp.float32), 0.5, 1.5),
        "up_first": normal_values(arg_keys[2], (D, FF), D ** -0.5, 0.1875, ((0, 32), (1, 8)), jnp.float32),
        "down_first": normal_values(arg_keys[3], (FF, D), FF ** -0.5, 0.09375, ((0, 8), (1, 32)), jnp.float32),
        "gain_second": jnp.clip(1.0 + 0.1 * jax.random.normal(arg_keys[4], (D,), jnp.float32), 0.5, 1.5),
        "up_second": normal_values(arg_keys[5], (D, FF), D ** -0.5, 0.1875, ((0, 32), (1, 8)), jnp.float32),
        "down_second": normal_values(arg_keys[6], (FF, D), FF ** -0.5, 0.09375, ((0, 8), (1, 32)), jnp.float32),
    }


EPS = 1e-06
RESIDUAL = 0.25

def sublayer(stream, norm_gain, w_up, w_down):
    floated = stream.astype(jnp.float32)
    squares = lax.optimization_barrier(jnp.sum(floated * floated, axis=1, keepdims=True))
    factor = jax.lax.rsqrt(squares / D + EPS)
    normed = (floated * factor * norm_gain.astype(jnp.float32)).astype(jnp.bfloat16)
    preact = jnp.dot(normed, w_up.astype(jnp.bfloat16), preferred_element_type=jnp.float32)
    activated = jnp.square(jax.nn.relu(preact)).astype(jnp.bfloat16)
    branch = jnp.dot(activated, w_down.astype(jnp.bfloat16), preferred_element_type=jnp.float32)
    return (RESIDUAL * floated + branch).astype(jnp.bfloat16)

def reference(stream, gain_first, up_first, down_first, gain_second, up_second, down_second):
    middle = sublayer(stream, gain_first, up_first, down_first)
    return sublayer(middle, gain_second, up_second, down_second)
```

```python
import jax
import jax.numpy as jnp
from jax import lax
from jax.experimental import pallas as pl
from jax.experimental.pallas import tpu as pltpu
from jax.sharding import PartitionSpec as P

D = 1024
EPS = 1e-06
RESIDUAL = 0.25
RA, CB = 32, 8
HALF = 64


def block_diagonal(packed, left):
    rolled = pltpu.roll(packed, HALF, 1)
    zero = jnp.zeros_like(packed)
    return jnp.concatenate(
        [
            jnp.where(left, packed, zero),
            jnp.where(left, rolled, zero),
            jnp.where(left, zero, rolled),
            jnp.where(left, zero, packed),
        ],
        axis=0,
    )


def kernel(
    stream_hbm, gain_a, up_a, down_a, gain_b, up_b, down_b, out_ref,
    stream_v, gain_v, up_v, down_v, upt_v, part_send, part_recv, act_send, act_recv, x_send, x_recv,
    load_sem, part_ss, part_rs, act_ss, act_rs, x_ss, x_rs,
):
    me = lax.axis_index("ra")
    col = lax.axis_index("cb")
    barrier = pltpu.get_barrier_semaphore()

    @pl.loop(1, RA)
    def _(step):
        pl.semaphore_signal(barrier, inc=1, device_id={"ra": lax.rem(me + step, RA)})

    @pl.loop(1, CB)
    def _(step):
        pl.semaphore_signal(barrier, inc=1, device_id={"cb": lax.rem(col + step, CB)})

    loads = [
        pltpu.make_async_copy(stream_hbm, stream_v, load_sem.at[0]),
        pltpu.make_async_copy(gain_a, gain_v.at[0], load_sem.at[1]),
        pltpu.make_async_copy(up_a, up_v.at[0], load_sem.at[2]),
        pltpu.make_async_copy(down_a, down_v.at[0], load_sem.at[3]),
        pltpu.make_async_copy(gain_b, gain_v.at[1], load_sem.at[4]),
        pltpu.make_async_copy(up_b, up_v.at[1], load_sem.at[5]),
        pltpu.make_async_copy(down_b, down_v.at[1], load_sem.at[6]),
    ]
    for load in loads:
        load.start()

    left = lax.broadcasted_iota(jnp.int32, (16, 128), 1) < HALF

    def prepare_up(layer):
        rows = up_v[layer].astype(jnp.bfloat16).astype(jnp.float32)
        stacked = jnp.concatenate([rows[:, :256], rows[:, 256:]], axis=0)
        gain = gain_v[layer]
        gains = jnp.concatenate([gain, gain], axis=1)
        upt_v[layer] = (stacked.T * gains).astype(jnp.bfloat16)

    def up_partial(layer, packed):
        blocks = block_diagonal(packed, left)
        squares = jnp.sum(blocks * blocks, axis=0, keepdims=True)
        high = squares.astype(jnp.bfloat16)
        low = (squares - high.astype(jnp.float32)).astype(jnp.bfloat16)
        pair = jnp.where(
            lax.broadcasted_iota(jnp.int32, (8, 128), 0) < 4,
            jnp.broadcast_to(high.astype(jnp.float32), (8, 128)),
            jnp.broadcast_to(low.astype(jnp.float32), (8, 128)),
        )
        partial = jnp.dot(upt_v[layer], blocks.astype(jnp.bfloat16), preferred_element_type=jnp.float32)
        tiles = jnp.concatenate(
            [partial.reshape(RA, 8, 128), jnp.broadcast_to(pair[None], (RA, 8, 128))], axis=1
        )
        part_send[layer] = tiles.astype(jnp.bfloat16)

    loads[0].wait()
    loads[1].wait()
    loads[2].wait()
    prepare_up(0)
    u_left = stream_v[...].astype(jnp.float32)
    u_both = jnp.concatenate([u_left, u_left], axis=1)
    packed = jnp.where(left, u_both[:16], u_both[16:])
    up_partial(0, packed)

    for layer in range(2):
        if layer == 0:
            pl.semaphore_wait(barrier, RA - 1 + CB - 1)
        part_recv[layer, me] = part_send[layer, me]

        @pl.loop(1, RA)
        def _(step):
            other = lax.rem(me + step, RA)
            pltpu.make_async_remote_copy(
                src_ref=part_send.at[layer, other],
                dst_ref=part_recv.at[layer, me],
                send_sem=part_ss.at[layer],
                recv_sem=part_rs.at[layer],
                device_id={"ra": other},
            ).start()

        if layer == 0:
            for load in loads[3:]:
                load.wait()
            prepare_up(1)
        down = down_v[layer].astype(jnp.bfloat16)
        down = jnp.concatenate([down[:, :256], down[:, 256:]], axis=0)

        arrived = part_recv.at[layer, pl.ds(0, RA - 1)]
        pltpu.make_async_copy(arrived, arrived, part_rs.at[layer]).wait()
        total = jnp.sum(part_recv[layer].astype(jnp.float32), axis=0)
        squares = total[8:9] + total[12:13]
        factor = lax.rsqrt(squares / D + EPS)
        preact = total[:8] * factor
        act_send[layer] = jnp.square(jnp.maximum(preact, 0.0)).astype(jnp.bfloat16)
        act_recv[layer, me] = act_send[layer]

        @pl.loop(1, RA)
        def _(step):
            other = lax.rem(me + step, RA)
            pltpu.make_async_remote_copy(
                src_ref=act_send.at[layer],
                dst_ref=act_recv.at[layer, me],
                send_sem=act_ss.at[layer],
                recv_sem=act_rs.at[layer],
                device_id={"ra": other},
            ).start()

        arrived = act_recv.at[layer, pl.ds(0, RA - 1)]
        pltpu.make_async_copy(arrived, arrived, act_rs.at[layer]).wait()
        activated = act_recv[layer].astype(jnp.float32).reshape(256, 128).astype(jnp.bfloat16)
        both = jnp.dot(down, activated, preferred_element_type=jnp.float32)
        straight = jnp.where(left, both[:16], both[48:])
        crossed = jnp.where(left, both[16:32], both[32:48])
        branch = straight + pltpu.roll(crossed, HALF, 1)
        x_send[layer] = branch.astype(jnp.bfloat16)
        x_recv[layer, col] = x_send[layer]

        @pl.loop(1, CB)
        def _(step):
            other = lax.rem(col + step, CB)
            pltpu.make_async_remote_copy(
                src_ref=x_send.at[layer],
                dst_ref=x_recv.at[layer, col],
                send_sem=x_ss.at[layer],
                recv_sem=x_rs.at[layer],
                device_id={"cb": other},
            ).start()

        arrived = x_recv.at[layer, pl.ds(0, CB - 1)]
        pltpu.make_async_copy(arrived, arrived, x_rs.at[layer]).wait()
        summed = jnp.sum(x_recv[layer].astype(jnp.float32), axis=0)
        packed = (RESIDUAL * packed + summed).astype(jnp.bfloat16).astype(jnp.float32)
        if layer == 0:
            up_partial(1, packed)

    rolled = pltpu.roll(packed, HALF, 1)
    result = jnp.concatenate([packed, rolled], axis=0)
    out_ref[...] = result[:, :HALF].astype(jnp.bfloat16)

    for layer in range(2):
        sent = part_recv.at[layer, pl.ds(0, RA - 1)]
        pltpu.make_async_copy(sent, sent, part_ss.at[layer]).wait()
        sent = act_recv.at[layer, pl.ds(0, RA - 1)]
        pltpu.make_async_copy(sent, sent, act_ss.at[layer]).wait()
        sent = x_recv.at[layer, pl.ds(0, CB - 1)]
        pltpu.make_async_copy(sent, sent, x_ss.at[layer]).wait()


def local(stream, gain_first, up_first, down_first, gain_second, up_second, down_second):
    call = pl.pallas_call(
        kernel,
        out_shape=jax.ShapeDtypeStruct((32, 64), jnp.bfloat16),
        in_specs=[pl.BlockSpec(memory_space=pl.ANY)] * 7,
        out_specs=pl.BlockSpec(memory_space=pltpu.VMEM),
        scratch_shapes=[
            pltpu.VMEM((32, 64), jnp.bfloat16),
            pltpu.VMEM((2, 1, 32), jnp.float32),
            pltpu.VMEM((2, 32, 512), jnp.float32),
            pltpu.VMEM((2, 32, 512), jnp.float32),
            pltpu.VMEM((2, 256, 64), jnp.bfloat16),
            pltpu.VMEM((2, RA, 16, 128), jnp.bfloat16),
            pltpu.VMEM((2, RA, 16, 128), jnp.bfloat16),
            pltpu.VMEM((2, 8, 128), jnp.bfloat16),
            pltpu.VMEM((2, RA, 8, 128), jnp.bfloat16),
            pltpu.VMEM((2, 16, 128), jnp.bfloat16),
            pltpu.VMEM((2, CB, 16, 128), jnp.bfloat16),
            pltpu.SemaphoreType.DMA((7,)),
        ]
        + [pltpu.SemaphoreType.DMA((2,))] * 6,
        compiler_params=pltpu.CompilerParams(collective_id=0, has_side_effects=True),
    )
    out = call(
        stream.T, gain_first[None], up_first, down_first.T, gain_second[None], up_second, down_second.T
    )
    return out.T


def solution(mesh):
    in_specs = (P(None, "ra"), P("ra"), P("ra", "cb"), P("cb", "ra"), P("ra"), P("ra", "cb"), P("cb", "ra"))
    return jax.shard_map(local, mesh=mesh, in_specs=in_specs, out_specs=P(None, "ra"), check_vma=False)
```

```python
import jax
import jax.numpy as jnp
from jax import lax
from jax.experimental import pallas as pl
from jax.experimental.pallas import tpu as pltpu
from jax.sharding import PartitionSpec as P

D = 1024
EPS = 1e-06
RESIDUAL = 0.25
BF = jnp.bfloat16
F32 = jnp.float32


def nt(a, b):
    return lax.dot_general(a, b, (((1,), (1,)), ((), ())), preferred_element_type=F32)


def nn(a, b):
    return jnp.dot(a, b, preferred_element_type=F32)


def lanes(shape):
    return lax.broadcasted_iota(jnp.int32, shape, len(shape) - 1)


def packed_of(both):
    return jnp.where(lanes((16, 128)) < 64, both[:16], both[16:])


def kernel(
    stream_h, gain_a, up_a, down_a, gain_b, up_b, down_b, out_ref,
    stream_v, gain_v, up_v, down_v,
    up1, down1s, up2s, down2,
    ps, pr, ys, yr, down1, up2y, up2, xs, xr, ms, mr, acts, actr, fs, fr, rs, rr,
    load_sem, give_ss, give_rs, ps_s, pr_s, ys_s, yr_s, d1_ss, d1_rs, u1_ss, u1_rs, u2_ss, u2_rs,
    xs_s, xr_s, ms_s, mr_s, as_s, ar_s, fs_s, fr_s, rs_s, rr_s,
):
    ra, cb = lax.axis_index("ra"), lax.axis_index("cb")
    z, y = ra // 4, ra % 4
    x, c = cb // 2, cb % 2
    barrier = pltpu.get_barrier_semaphore()
    loads = [
        pltpu.make_async_copy(src, dst, load_sem.at[k])
        for k, (src, dst) in enumerate(
            [
                (stream_h, stream_v),
                (gain_a, gain_v.at[0]),
                (up_a, up_v.at[0]),
                (down_a, down_v.at[0]),
                (gain_b, gain_v.at[1]),
                (up_b, up_v.at[1]),
                (down_b, down_v.at[1]),
            ]
        )
    ]

    def at(dz, dy, dx, core):
        return {"ra": ((z + dz) % 8) * 4 + (y + dy) % 4, "cb": ((x + dx) % 4) * 2 + core}

    def send(src, dst, ss, rsem, where):
        pltpu.make_async_remote_copy(
            src_ref=src, dst_ref=dst, send_sem=ss, recv_sem=rsem, device_id=where
        ).start()

    def drain(ref, sem):
        pltpu.make_async_copy(ref, ref, sem).wait()

    def hello(where):
        pl.semaphore_signal(barrier, inc=1, device_id=where)

    def prepare_up1():
        up1[c] = up_v[0].astype(BF)

    def prepare_down1():
        down1s[c] = down_v[0].astype(BF)

    def prepare_up2():
        eye = lax.broadcasted_iota(jnp.int32, (32, 32), 0) == lanes((32, 32))
        column = jnp.sum(jnp.where(eye, gain_v[1], 0.0), axis=1, keepdims=True)
        scaled = (up_v[1].astype(BF).astype(F32) * column).astype(BF)
        for k in range(4):
            up2s[k, c] = scaled[:, 128 * k : 128 * k + 128]

    def prepare_down2():
        down2[c] = down_v[1].astype(BF)

    def finish():
        total = jnp.sum(fr[...].astype(F32), axis=0) + rr[...]
        total = total.astype(BF).astype(F32)
        rolled = pltpu.roll(total, 64, 1)
        out_ref[...] = jnp.concatenate([total, rolled], axis=0)[:, :64].astype(BF)

    @pl.when(c == 0)
    def _():
        for dx in range(4):
            hello(at(0, 0, dx, 1))
        for load in loads[2:]:
            load.start()
        loads[2].wait()
        prepare_up1()
        pl.semaphore_wait(barrier, 1)
        partner = at(0, 0, 0, 1)
        send(up1.at[0], up1.at[0], give_ss.at[0], give_rs.at[0], partner)
        loads[3].wait()
        prepare_down1()
        send(down1s.at[0], down1s.at[0], give_ss.at[1], give_rs.at[1], partner)
        loads[4].wait()
        loads[5].wait()
        prepare_up2()
        send(up2s.at[:, 0], up2s.at[:, 0], give_ss.at[2], give_rs.at[2], partner)
        loads[6].wait()
        prepare_down2()
        send(down2.at[0], down2.at[0], give_ss.at[3], give_rs.at[3], partner)
        drain(up1.at[0], give_ss.at[0])
        drain(down1s.at[0], give_ss.at[1])
        drain(up2s.at[:, 0], give_ss.at[2])
        drain(down2.at[0], give_ss.at[3])
        drain(rr, rr_s)
        drain(fr, fr_s)
        finish()

    @pl.when(c == 1)
    def _():
        far = (4, 3, 5, 2, 6, 1, 7)
        for dz in far:
            hello(at(dz, 0, 0, 1))
        for d in (2, 1, 3):
            hello(at(0, d, 0, 1))
            hello(at(0, 0, d, 1))
        hello(at(0, 0, 0, 0))
        for load in loads:
            load.start()

        for k in range(2):
            loads[k].wait()
        u = stream_v[...].astype(F32).T
        place = lanes((32, 128)) == 32 * (z % 4) + lax.broadcasted_iota(jnp.int32, (32, 128), 0)
        tile = nn(u.astype(BF), place.astype(F32).astype(BF))
        ps[:, :, 1024:] = tile.reshape(8, 8, 128).astype(BF)
        lhs = (u * gain_v[0]).astype(BF)
        loads[2].wait()
        prepare_up1()
        ps[:, :, 512:1024] = nn(lhs, up1[1]).reshape(8, 8, 512).astype(BF)
        drain(up1.at[0], give_rs.at[0])
        ps[:, :, :512] = nn(lhs, up1[0]).reshape(8, 8, 512).astype(BF)

        pl.semaphore_wait(barrier, 17)
        for dz in far:
            send(ps.at[(z + dz) % 8], pr.at[z], ps_s, pr_s, at(dz, 0, 0, 1))
        pr[z] = ps[z]
        loads[3].wait()
        prepare_down1()
        for dz in far:
            send(down1s.at[1], down1.at[1, z], d1_ss, d1_rs, at(dz, 0, 0, 1))
        loads[4].wait()
        loads[5].wait()
        prepare_up2()
        drain(up2s.at[:, 0], give_rs.at[2])
        for dy in (2, 1, 3):
            send(up2s.at[(y + dy) % 4], up2y.at[y], u1_ss, u1_rs, at(0, dy, 0, 1))
        drain(down1s.at[0], give_rs.at[1])
        for dz in far:
            send(down1s.at[0], down1.at[0, z], d1_ss, d1_rs, at(dz, 0, 0, 1))
        up2y[y] = up2s[y]
        down1[0, z] = down1s[0]
        down1[1, z] = down1s[1]

        drain(pr.at[pl.ds(0, 7)], pr_s)
        partial = jnp.sum(pr[:, :, :1024].astype(F32), axis=0)
        u_own = jnp.concatenate(
            [
                jnp.sum(pr[0:4, :, 1024:].astype(F32), axis=0),
                jnp.sum(pr[4:8, :, 1024:].astype(F32), axis=0),
            ],
            axis=1,
        )
        squares = jnp.sum(u_own * u_own, axis=1, keepdims=True)
        high = squares.astype(BF).astype(F32)
        ys[:, :1024] = partial.astype(BF)
        ys[:, 1024:] = jnp.where(lanes((8, 128)) < 64, high, squares - high).astype(BF)
        for dy in (2, 1, 3):
            send(ys, yr.at[y], ys_s, yr_s, at(0, dy, 0, 1))
        yr[y] = ys[...]

        drain(up2y.at[pl.ds(0, 3)], u1_rs)
        for dz in far:
            send(up2y, up2.at[z], u2_ss, u2_rs, at(dz, 0, 0, 1))
        up2[z] = up2y[...]

        drain(yr.at[pl.ds(0, 3)], yr_s)
        preact = jnp.sum(yr[...].astype(F32), axis=0)
        squares = jnp.sum(preact[:, 1024:], axis=1, keepdims=True) / 64
        factor = lax.rsqrt(squares / D + EPS)
        act = jnp.square(jnp.maximum(preact[:, :1024] * factor, 0.0)).astype(BF)

        drain(down1.at[:, pl.ds(0, 7)], d1_rs)
        branch = nt(act[:, :512], down1[0].reshape(256, 512)) + nt(act[:, 512:], down1[1].reshape(256, 512))
        share = jnp.where(x == 0, RESIDUAL, 0.0)
        xs[...] = (branch + share * u_own).astype(BF)
        for dy in (2, 1, 3, 0):
            for dx in (2, 1, 3, 0):
                if dy or dx:
                    send(xs, xr.at[4 * y + x], xs_s, xr_s, at(0, dy, dx, 1))
        xr[4 * y + x] = xs[...]
        loads[6].wait()
        prepare_down2()
        drain(down2.at[0], give_rs.at[3])

        drain(xr.at[pl.ds(0, 15)], xr_s)
        middle = jnp.sum(xr[...].astype(F32).reshape(4, 4, 8, 256), axis=1).astype(BF).astype(F32)
        middle = jnp.concatenate([middle[k] for k in range(4)], axis=1)
        squares = jnp.sum(middle * middle, axis=1, keepdims=True)
        factor = lax.rsqrt(squares / D + EPS)
        middle = middle.astype(BF)
        drain(up2.at[pl.ds(0, 7)], u2_rs)
        pre = []
        for k in range(2):
            rows = jnp.concatenate([up2[a, b, k] for b in range(4) for a in range(8)], axis=0)
            pre.append(nn(middle, rows))
        act = jnp.square(jnp.maximum(jnp.concatenate(pre, axis=1) * factor, 0.0))
        acts[...] = act.astype(BF)

        @pl.loop(1, 32)
        def _(step):
            send(acts, actr.at[8 * y + z], as_s, ar_s, at(step // 4, step % 4, 0, 1))

        actr[8 * y + z] = acts[...]
        own = jnp.sum(xr[pl.ds(4 * y, 4)].astype(F32), axis=0).astype(BF)
        ms[0] = own[:, :128]
        ms[1] = own[:, 128:]
        for dz in far:
            send(ms.at[((z + dz) % 8) // 4], mr.at[z], ms_s, mr_s, at(dz, 0, 0, 1))
        mr[z] = ms[z // 4]
        drain(mr.at[pl.ds(0, 7)], mr_s)
        mid = mr[...].astype(F32).reshape(64, 128).astype(BF)
        mid = jnp.concatenate([mid, mid], axis=0)
        rs[...] = RESIDUAL * packed_of(nt(place.astype(F32).astype(BF), mid))
        send(rs, rr, rs_s, rr_s, at(0, 0, 0, 0))
        rr[...] = rs[...]

        drain(actr.at[pl.ds(0, 31)], ar_s)
        weights = jnp.concatenate(
            [down2[k, :, 128 * b : 128 * b + 128] for b in range(4) for k in range(2)], axis=1
        )
        gathered = actr[...].astype(F32).reshape(4, 64, 256)
        gathered = jnp.concatenate([gathered[b] for b in range(4)], axis=1).astype(BF)
        gathered = jnp.concatenate([gathered, gathered], axis=0)
        fs[...] = packed_of(nt(weights, gathered)).astype(BF)
        for dx in (2, 1, 3):
            send(fs, fr.at[x], fs_s, fr_s, at(0, 0, dx, 0))
            send(fs, fr.at[x], fs_s, fr_s, at(0, 0, dx, 1))
        send(fs, fr.at[x], fs_s, fr_s, at(0, 0, 0, 0))
        fr[x] = fs[...]
        drain(fr.at[pl.ds(0, 3)], fr_s)
        finish()

        drain(ps.at[pl.ds(0, 7)], ps_s)
        drain(down1.at[:, pl.ds(0, 7)], d1_ss)
        drain(up2y.at[pl.ds(0, 3)], u1_ss)
        drain(yr.at[pl.ds(0, 3)], ys_s)
        drain(up2.at[pl.ds(0, 7)], u2_ss)
        drain(xr.at[pl.ds(0, 15)], xs_s)
        drain(actr.at[pl.ds(0, 31)], as_s)
        drain(mr.at[pl.ds(0, 7)], ms_s)
        drain(rr, rs_s)
        drain(xr.at[pl.ds(0, 7)], fs_s)


def local(stream, gain_first, up_first, down_first, gain_second, up_second, down_second):
    vmem = [
        ((32, 64), BF), ((2, 1, 32), F32), ((2, 32, 512), F32), ((2, 32, 512), F32),
        ((2, 32, 512), BF), ((2, 32, 512), BF), ((4, 2, 32, 128), BF), ((2, 32, 512), BF),
        ((8, 8, 1152), BF), ((8, 8, 1152), BF), ((8, 1152), BF), ((4, 8, 1152), BF),
        ((2, 8, 32, 512), BF), ((4, 2, 32, 128), BF), ((8, 4, 2, 32, 128), BF),
        ((8, 256), BF), ((16, 8, 256), BF), ((2, 8, 128), BF), ((8, 8, 128), BF),
        ((8, 256), BF), ((32, 8, 256), BF), ((16, 128), BF), ((4, 16, 128), BF),
        ((16, 128), F32), ((16, 128), F32),
    ]
    dma = pltpu.SemaphoreType.DMA
    call = pl.pallas_call(
        kernel,
        out_shape=jax.ShapeDtypeStruct((32, 64), BF),
        in_specs=[pl.BlockSpec(memory_space=pl.ANY)] * 7,
        out_specs=pl.BlockSpec(memory_space=pltpu.VMEM),
        scratch_shapes=[pltpu.VMEM(*v) for v in vmem] + [dma((7,)), dma((4,)), dma((4,))] + [dma(())] * 20,
        compiler_params=pltpu.CompilerParams(collective_id=0, has_side_effects=True),
    )
    out = call(
        stream.T, gain_first[None], up_first, down_first.T, gain_second[None], up_second, down_second.T
    )
    return out.T


def solution(mesh):
    in_specs = (P(None, "ra"), P("ra"), P("ra", "cb"), P("cb", "ra"), P("ra"), P("ra", "cb"), P("cb", "ra"))
    return jax.shard_map(local, mesh=mesh, in_specs=in_specs, out_specs=P(None, "ra"), check_vma=False)
```

```python
import jax
import jax.numpy as jnp
from jax import lax
from jax.experimental import pallas as pl
from jax.experimental.pallas import tpu as pltpu
from jax.sharding import PartitionSpec as P

D = 1024
EPS = 1e-06
RESIDUAL = 0.25
BF = jnp.bfloat16
F32 = jnp.float32


def nt(a, b):
    return lax.dot_general(a, b, (((1,), (1,)), ((), ())), preferred_element_type=F32)


def nn(a, b):
    return jnp.dot(a, b, preferred_element_type=F32)


def lanes(shape):
    return lax.broadcasted_iota(jnp.int32, shape, len(shape) - 1)


def packed_of(both):
    return jnp.where(lanes((16, 128)) < 64, both[:16], both[16:])


def kernel(
    stream_h, gain_a, up_a, down_a, gain_b, up_b, down_b, out_ref,
    stream_v, gain_v, up_v, down_v,
    down1s, up2s, down2,
    ps, pr0, pr1, ys, yr, down1, up2y, up2, xs, xr, ms, mr, acts, actr, fs, fr, rs, rr,
    load_sem, give_ss, give_rs, ps_s, pr0_s, pr1_s, ys_s, yr_s, d1a_ss, d1a_rs, d1b_ss, d1b_rs,
    u1_ss, u1_rs, u2a_ss, u2a_rs, u2b_ss, u2b_rs,
    xs_s, xr_s, ms_s, mr_s, as_s, ar_s, fs_s, fr_s, rs_s, rr_s,
):
    ra, cb = lax.axis_index("ra"), lax.axis_index("cb")
    z, y = lax.div(ra, 4), lax.rem(ra, 4)
    x, c = lax.div(cb, 2), lax.rem(cb, 2)
    far = (4, 3, 5, 2, 6, 1, 7)
    near = (2, 6, 1, 7)
    barrier = pltpu.get_barrier_semaphore()
    loads = [
        pltpu.make_async_copy(src, dst, load_sem.at[k])
        for k, (src, dst) in enumerate(
            [
                (stream_h, stream_v),
                (gain_a, gain_v.at[0]),
                (up_a, up_v.at[0]),
                (down_a, down_v.at[0]),
                (gain_b, gain_v.at[1]),
                (up_b, up_v.at[1]),
                (down_b, down_v.at[1]),
            ]
        )
    ]

    def at(dz, dy, dx, core):
        return {"ra": lax.rem(z + dz, 8) * 4 + lax.rem(y + dy, 4), "cb": lax.rem(x + dx, 4) * 2 + core}

    def send(src, dst, ss, rsem, where):
        pltpu.make_async_remote_copy(
            src_ref=src, dst_ref=dst, send_sem=ss, recv_sem=rsem, device_id=where
        ).start()

    def drain(ref, sem):
        pltpu.make_async_copy(ref, ref, sem).wait()

    def hello(where):
        pl.semaphore_signal(barrier, inc=1, device_id=where)

    def first_up():
        loads[0].wait()
        loads[1].wait()
        u = stream_v[...].astype(F32).T
        loads[2].wait()
        part = nn((u * gain_v[0]).astype(BF), up_v[0].astype(BF))
        ps[:, :, :512] = part.reshape(8, 8, 512).astype(BF)
        return u

    def prepare_up2():
        eye = lax.broadcasted_iota(jnp.int32, (32, 32), 0) == lanes((32, 32))
        column = jnp.sum(jnp.where(eye, gain_v[1], 0.0), axis=1, keepdims=True)
        scaled = (up_v[1].astype(BF).astype(F32) * column).astype(BF)
        for k in range(4):
            up2s[k, c] = scaled[:, 128 * k : 128 * k + 128]

    def prepare_down2():
        down2[c] = down_v[1].astype(BF)

    def finish():
        total = jnp.sum(fr[...].astype(F32), axis=0) + rr[...]
        total = total.astype(BF).astype(F32)
        rolled = pltpu.roll(total, 64, 1)
        out_ref[...] = jnp.concatenate([total, rolled], axis=0)[:, :64].astype(BF)

    for load in loads[:3]:
        load.start()

    @pl.when(c == 0)
    def _():
        for dx in range(4):
            hello(at(0, 0, dx, 1))
        for load in loads[3:]:
            load.start()
        first_up()
        pl.semaphore_wait(barrier, 8)
        for dz in far + (0,):
            send(ps.at[lax.rem(z + dz, 8), :, pl.ds(0, 512)], pr0.at[z], ps_s, pr0_s, at(dz, 0, 0, 1))
        partner = at(0, 0, 0, 1)
        loads[3].wait()
        down1s[...] = down_v[0].astype(BF)
        for dz in near + (0,):
            send(down1s, down1.at[z], d1a_ss, d1a_rs, at(dz, 0, 0, 1))
        loads[4].wait()
        loads[5].wait()
        prepare_up2()
        send(up2s.at[:, 0], up2s.at[:, 0], give_ss.at[0], give_rs.at[0], partner)
        loads[6].wait()
        prepare_down2()
        send(down2.at[0], down2.at[0], give_ss.at[1], give_rs.at[1], partner)
        drain(pr0, ps_s)
        drain(down1.at[pl.ds(0, 5)], d1a_ss)
        drain(up2s.at[:, 0], give_ss.at[0])
        drain(down2.at[0], give_ss.at[1])
        drain(rr, rr_s)
        drain(fr, fr_s)
        finish()

    @pl.when(c == 1)
    def _():
        for dz in far:
            hello(at(dz, 0, 0, 1))
            hello(at(dz, 0, 0, 0))
        for d in (2, 1, 3):
            hello(at(0, d, 0, 1))
            hello(at(0, 0, d, 1))
        hello(at(0, 0, 0, 0))
        for load in loads[3:]:
            load.start()

        u = first_up()
        place = lanes((32, 128)) == 32 * lax.rem(z, 4) + lax.broadcasted_iota(jnp.int32, (32, 128), 0)
        place = place.astype(F32).astype(BF)
        ps[:, :, 512:] = nn(u.astype(BF), place).reshape(8, 8, 128).astype(BF)

        pl.semaphore_wait(barrier, 17)
        for dz in far:
            send(ps.at[lax.rem(z + dz, 8)], pr1.at[z], ps_s, pr1_s, at(dz, 0, 0, 1))
        loads[3].wait()
        down1s[...] = down_v[0].astype(BF)
        for dz in near:
            send(down1s, down1.at[8 + z], d1a_ss, d1a_rs, at(dz, 0, 0, 1))
        pr1[z] = ps[z]
        loads[4].wait()
        loads[5].wait()
        prepare_up2()
        drain(up2s.at[:, 0], give_rs.at[0])
        for dy in (2, 1, 3):
            send(up2s.at[lax.rem(y + dy, 4)], up2y.at[y], u1_ss, u1_rs, at(0, dy, 0, 1))
        up2y[y] = up2s[y]
        down1[8 + z] = down1s[...]

        drain(pr0, pr0_s)
        drain(pr1.at[pl.ds(0, 7)], pr1_s)
        partial = [jnp.sum(pr0[...].astype(F32), axis=0), jnp.sum(pr1[:, :, :512].astype(F32), axis=0)]
        u_own = jnp.concatenate(
            [
                jnp.sum(pr1[0:4, :, 512:].astype(F32), axis=0),
                jnp.sum(pr1[4:8, :, 512:].astype(F32), axis=0),
            ],
            axis=1,
        )
        squares = jnp.sum(u_own * u_own, axis=1, keepdims=True)
        high = squares.astype(BF).astype(F32)
        ys[:, :512] = partial[0].astype(BF)
        ys[:, 512:1024] = partial[1].astype(BF)
        ys[:, 1024:] = jnp.where(lanes((8, 128)) < 64, high, squares - high).astype(BF)
        for dy in (2, 1, 3):
            send(ys, yr.at[y], ys_s, yr_s, at(0, dy, 0, 1))
        yr[y] = ys[...]

        drain(up2y.at[pl.ds(0, 3)], u1_rs)
        for dz in near:
            send(up2y, up2.at[z], u2a_ss, u2a_rs, at(dz, 0, 0, 1))
        up2[z] = up2y[...]

        back, ahead = lax.rem(z + 6, 8), lax.rem(z + 2, 8)
        drain(down1.at[pl.ds(0, 9)], d1a_rs)
        for b, a in ((back, ahead), (back + 8, ahead + 8)):
            send(down1.at[b, pl.ds(0, 16)], down1.at[b, pl.ds(0, 16)], d1b_ss, d1b_rs, at(2, 0, 0, 1))
            send(down1.at[a, pl.ds(16, 16)], down1.at[a, pl.ds(16, 16)], d1b_ss, d1b_rs, at(6, 0, 0, 1))
            send(down1.at[b], down1.at[b], d1b_ss, d1b_rs, at(1, 0, 0, 1))
            send(down1.at[a], down1.at[a], d1b_ss, d1b_rs, at(7, 0, 0, 1))

        drain(yr.at[pl.ds(0, 3)], yr_s)
        preact = jnp.sum(yr[...].astype(F32), axis=0)
        squares = jnp.sum(preact[:, 1024:], axis=1, keepdims=True) / 64
        factor = lax.rsqrt(squares / D + EPS)
        act = jnp.square(jnp.maximum(preact[:, :1024] * factor, 0.0)).astype(BF)

        drain(up2.at[pl.ds(0, 4)], u2a_rs)
        send(up2.at[back, pl.ds(0, 2)], up2.at[back, pl.ds(0, 2)], u2b_ss, u2b_rs, at(2, 0, 0, 1))
        send(up2.at[ahead, pl.ds(2, 2)], up2.at[ahead, pl.ds(2, 2)], u2b_ss, u2b_rs, at(6, 0, 0, 1))
        send(up2.at[back], up2.at[back], u2b_ss, u2b_rs, at(1, 0, 0, 1))
        send(up2.at[ahead], up2.at[ahead], u2b_ss, u2b_rs, at(7, 0, 0, 1))

        drain(down1.at[pl.ds(0, 6)], d1b_rs)
        branch = nt(act[:, :512], down1[:8].reshape(256, 512)) + nt(act[:, 512:], down1[8:].reshape(256, 512))
        share = jnp.where(x == 0, RESIDUAL, 0.0)
        xs[...] = (branch + share * u_own).astype(BF)
        for dy in (2, 1, 3, 0):
            for dx in (2, 1, 3, 0):
                if dy or dx:
                    send(xs, xr.at[4 * y + x], xs_s, xr_s, at(0, dy, dx, 1))
        xr[4 * y + x] = xs[...]
        loads[6].wait()
        prepare_down2()
        drain(down2.at[0], give_rs.at[1])

        drain(xr.at[pl.ds(0, 15)], xr_s)
        middle = jnp.sum(xr[...].astype(F32).reshape(4, 4, 8, 256), axis=1).astype(BF).astype(F32)
        middle = jnp.concatenate([middle[k] for k in range(4)], axis=1)
        squares = jnp.sum(middle * middle, axis=1, keepdims=True)
        factor = lax.rsqrt(squares / D + EPS)
        middle = middle.astype(BF)
        drain(up2.at[pl.ds(0, 3)], u2b_rs)
        pre = []
        for k in range(2):
            rows = jnp.concatenate([up2[a, b, k] for b in range(4) for a in range(8)], axis=0)
            pre.append(nn(middle, rows))
        act = jnp.square(jnp.maximum(jnp.concatenate(pre, axis=1) * factor, 0.0))
        acts[...] = act.astype(BF)

        @pl.loop(1, 32)
        def _(step):
            send(acts, actr.at[8 * y + z], as_s, ar_s, at(lax.div(step, 4), lax.rem(step, 4), 0, 1))

        actr[8 * y + z] = acts[...]
        own = jnp.sum(xr[pl.ds(4 * y, 4)].astype(F32), axis=0).astype(BF)
        ms[0] = own[:, :128]
        ms[1] = own[:, 128:]
        for dz in far:
            send(ms.at[lax.div(lax.rem(z + dz, 8), 4)], mr.at[z], ms_s, mr_s, at(dz, 0, 0, 1))
        mr[z] = ms[lax.div(z, 4)]
        drain(mr.at[pl.ds(0, 7)], mr_s)
        mid = mr[...].astype(F32).reshape(64, 128).astype(BF)
        mid = jnp.concatenate([mid, mid], axis=0)
        rs[...] = RESIDUAL * packed_of(nt(place, mid))
        send(rs, rr, rs_s, rr_s, at(0, 0, 0, 0))
        rr[...] = rs[...]

        drain(actr.at[pl.ds(0, 31)], ar_s)
        weights = jnp.concatenate(
            [down2[k, :, 128 * b : 128 * b + 128] for b in range(4) for k in range(2)], axis=1
        )
        gathered = actr[...].astype(F32).reshape(4, 64, 256)
        gathered = jnp.concatenate([gathered[b] for b in range(4)], axis=1).astype(BF)
        gathered = jnp.concatenate([gathered, gathered], axis=0)
        fs[...] = packed_of(nt(weights, gathered)).astype(BF)
        for dx in (2, 1, 3):
            send(fs, fr.at[x], fs_s, fr_s, at(0, 0, dx, 0))
            send(fs, fr.at[x], fs_s, fr_s, at(0, 0, dx, 1))
        send(fs, fr.at[x], fs_s, fr_s, at(0, 0, 0, 0))
        fr[x] = fs[...]
        drain(fr.at[pl.ds(0, 3)], fr_s)
        finish()

        drain(pr1.at[pl.ds(0, 7)], ps_s)
        drain(down1.at[pl.ds(0, 4)], d1a_ss)
        drain(down1.at[pl.ds(0, 6)], d1b_ss)
        drain(up2y.at[pl.ds(0, 3)], u1_ss)
        drain(yr.at[pl.ds(0, 3)], ys_s)
        drain(up2.at[pl.ds(0, 4)], u2a_ss)
        drain(up2.at[pl.ds(0, 3)], u2b_ss)
        drain(xr.at[pl.ds(0, 15)], xs_s)
        drain(actr.at[pl.ds(0, 31)], as_s)
        drain(mr.at[pl.ds(0, 7)], ms_s)
        drain(rr, rs_s)
        drain(xr.at[pl.ds(0, 7)], fs_s)


def local(stream, gain_first, up_first, down_first, gain_second, up_second, down_second):
    vmem = [
        ((32, 64), BF), ((2, 1, 32), F32), ((2, 32, 512), F32), ((2, 32, 512), F32),
        ((32, 512), BF), ((4, 2, 32, 128), BF), ((2, 32, 512), BF),
        ((8, 8, 640), BF), ((8, 8, 512), BF), ((8, 8, 640), BF), ((8, 1152), BF), ((4, 8, 1152), BF),
        ((16, 32, 512), BF), ((4, 2, 32, 128), BF), ((8, 4, 2, 32, 128), BF),
        ((8, 256), BF), ((16, 8, 256), BF), ((2, 8, 128), BF), ((8, 8, 128), BF),
        ((8, 256), BF), ((32, 8, 256), BF), ((16, 128), BF), ((4, 16, 128), BF),
        ((16, 128), F32), ((16, 128), F32),
    ]
    dma = pltpu.SemaphoreType.DMA
    call = pl.pallas_call(
        kernel,
        out_shape=jax.ShapeDtypeStruct((32, 64), BF),
        in_specs=[pl.BlockSpec(memory_space=pl.ANY)] * 7,
        out_specs=pl.BlockSpec(memory_space=pltpu.VMEM),
        scratch_shapes=[pltpu.VMEM(*v) for v in vmem] + [dma((7,)), dma((2,)), dma((2,))] + [dma(())] * 25,
        compiler_params=pltpu.CompilerParams(collective_id=0, has_side_effects=True),
    )
    out = call(
        stream.T, gain_first[None], up_first, down_first.T, gain_second[None], up_second, down_second.T
    )
    return out.T


def solution(mesh):
    in_specs = (P(None, "ra"), P("ra"), P("ra", "cb"), P("cb", "ra"), P("ra"), P("ra", "cb"), P("cb", "ra"))
    return jax.shard_map(local, mesh=mesh, in_specs=in_specs, out_specs=P(None, "ra"), check_vma=False)
```

```python
import jax
import jax.numpy as jnp
from jax import lax
from jax.experimental import pallas as pl
from jax.experimental.pallas import tpu as pltpu
from jax.sharding import PartitionSpec as P

D = 1024
EPS = 1e-06
RESIDUAL = 0.25
BF = jnp.bfloat16
F32 = jnp.float32


def nt(a, b):
    return lax.dot_general(a, b, (((1,), (1,)), ((), ())), preferred_element_type=F32)


def nn(a, b):
    return jnp.dot(a, b, preferred_element_type=F32)


def lanes(shape):
    return lax.broadcasted_iota(jnp.int32, shape, len(shape) - 1)


def packed_of(both):
    return jnp.where(lanes((16, 128)) < 64, both[:16], both[16:])


def kernel(
    stream_h, gain_a, up_a, down_a, gain_b, up_b, down_b, out_ref,
    stream_v, gain_v, up_v, down_v,
    down1s, up2s, down2,
    ps, pr0, pr1, ys, yr, down1, up2y, up2, xs, xr, ms, mr, acts, actr, fs, fr, rs, rr,
    load_sem, give_ss, give_rs, ps_s, pr0_s, pr1_s, ys_s, yr_s, d1a_ss, d1a_rs, d1b_ss, d1b_rs,
    u1_ss, u1_rs, u2a_ss, u2a_rs, u2b_ss, u2b_rs,
    xs_s, xr_s, ms_s, mr_s, as_s, ar_s, fs_s, fr_s, rs_s, rr_s, d1c_ss, d1c_rs, u2c_ss, u2c_rs, go,
):
    ra, cb = lax.axis_index("ra"), lax.axis_index("cb")
    z, y = lax.div(ra, 4), lax.rem(ra, 4)
    x, c = lax.div(cb, 2), lax.rem(cb, 2)
    far = (4, 3, 5, 2, 6, 1, 7)
    barrier = pltpu.get_barrier_semaphore()
    loads = [
        pltpu.make_async_copy(src, dst, load_sem.at[k])
        for k, (src, dst) in enumerate(
            [
                (stream_h, stream_v),
                (gain_a, gain_v.at[0]),
                (up_a, up_v.at[0]),
                (down_a, down_v.at[0]),
                (gain_b, gain_v.at[1]),
                (up_b, up_v.at[1]),
                (down_b, down_v.at[1]),
            ]
        )
    ]

    def at(dz, dy, dx, core):
        return {"ra": lax.rem(z + dz, 8) * 4 + lax.rem(y + dy, 4), "cb": lax.rem(x + dx, 4) * 2 + core}

    def send(src, dst, ss, rsem, where):
        pltpu.make_async_remote_copy(
            src_ref=src, dst_ref=dst, send_sem=ss, recv_sem=rsem, device_id=where
        ).start()

    def drain(ref, sem):
        pltpu.make_async_copy(ref, ref, sem).wait()

    def hello(where):
        pl.semaphore_signal(barrier, inc=1, device_id=where)

    def first_up():
        loads[0].wait()
        loads[1].wait()
        u = stream_v[...].astype(F32).T
        loads[2].wait()
        part = nn((u * gain_v[0]).astype(BF), up_v[0].astype(BF))
        ps[:, :, :512] = part.reshape(8, 8, 512).astype(BF)
        return u

    def prepare_up2():
        eye = lax.broadcasted_iota(jnp.int32, (32, 32), 0) == lanes((32, 32))
        loads[4].wait()
        loads[5].wait()
        column = jnp.sum(jnp.where(eye, gain_v[1], 0.0), axis=1, keepdims=True)
        scaled = (up_v[1].astype(BF).astype(F32) * column).astype(BF)
        for k in range(4):
            up2s[k] = scaled[:, 128 * k : 128 * k + 128]

    def prepare_down1():
        loads[3].wait()
        down1s[...] = down_v[0].astype(BF)

    def prepare_down2():
        down2[c] = down_v[1].astype(BF)

    def finish():
        total = jnp.sum(fr[...].astype(F32), axis=0) + rr[...]
        total = total.astype(BF).astype(F32)
        rolled = pltpu.roll(total, 64, 1)
        out_ref[...] = jnp.concatenate([total, rolled], axis=0)[:, :64].astype(BF)

    for load in loads[:3]:
        load.start()

    @pl.when(c == 0)
    def _():
        for dx in range(4):
            hello(at(0, 0, dx, 1))
        for load in loads[3:]:
            load.start()
        first_up()
        prepare_up2()
        prepare_down1()
        pl.semaphore_wait(barrier, 1)
        pl.semaphore_wait(go, 1)
        for dz in far + (0,):
            send(ps.at[lax.rem(z + dz, 8), :, pl.ds(0, 512)], pr0.at[z], ps_s, pr0_s, at(dz, 0, 0, 1))
        for dy in (2, 1, 3, 0):
            send(up2s.at[lax.rem(y + dy, 4)], up2y.at[y, 0], u1_ss, u1_rs, at(0, dy, 0, 1))
        for dz in (2, 6):
            send(down1s, down1.at[z], d1a_ss, d1a_rs, at(dz, 0, 0, 1))
        for dz in (1, 7, 0):
            send(down1s, down1.at[z], d1c_ss, d1c_rs, at(dz, 0, 0, 1))
        partner = at(0, 0, 0, 1)
        loads[6].wait()
        prepare_down2()
        send(down2.at[0], down2.at[0], give_ss, give_rs, partner)
        drain(pr0, ps_s)
        drain(down1.at[pl.ds(0, 2)], d1a_ss)
        drain(down1.at[pl.ds(0, 3)], d1c_ss)
        drain(up2s, u1_ss)
        drain(down2.at[0], give_ss)
        drain(rr, rr_s)
        drain(fr, fr_s)
        finish()

    @pl.when(c == 1)
    def _():
        for dz in far:
            hello(at(dz, 0, 0, 1))
        for d in (2, 1, 3):
            hello(at(0, d, 0, 1))
            hello(at(0, 0, d, 1))
        hello(at(0, 0, 0, 0))
        for load in loads[3:]:
            load.start()

        u = first_up()
        place = lanes((32, 128)) == 32 * lax.rem(z, 4) + lax.broadcasted_iota(jnp.int32, (32, 128), 0)
        place = place.astype(F32).astype(BF)
        ps[:, :, 512:] = nn(u.astype(BF), place).reshape(8, 8, 128).astype(BF)
        prepare_up2()
        prepare_down1()

        pl.semaphore_wait(barrier, 17)
        pl.semaphore_signal(go, inc=1, device_id=at(0, 0, 0, 0))
        for dz in far:
            send(ps.at[lax.rem(z + dz, 8)], pr1.at[z], ps_s, pr1_s, at(dz, 0, 0, 1))
        for dy in (2, 1, 3):
            send(up2s.at[lax.rem(y + dy, 4)], up2y.at[y, 1], u1_ss, u1_rs, at(0, dy, 0, 1))
        for dz in (2, 6):
            send(down1s, down1.at[8 + z], d1a_ss, d1a_rs, at(dz, 0, 0, 1))
        for dz in (1, 7):
            send(down1s, down1.at[8 + z], d1c_ss, d1c_rs, at(dz, 0, 0, 1))
        pr1[z] = ps[z]
        down1[8 + z] = down1s[...]
        up2y[y, 1] = up2s[y]
        drain(down1.at[pl.ds(0, 7), :, pl.ds(0, 128)], u1_rs)
        for dz in (2, 6):
            send(up2y, up2.at[z], u2a_ss, u2a_rs, at(dz, 0, 0, 1))
        for dz in (1, 7):
            send(up2y, up2.at[z], u2c_ss, u2c_rs, at(dz, 0, 0, 1))
        up2[z] = up2y[...]

        drain(pr0, pr0_s)
        drain(pr1.at[pl.ds(0, 7)], pr1_s)
        partial = [jnp.sum(pr0[...].astype(F32), axis=0), jnp.sum(pr1[:, :, :512].astype(F32), axis=0)]
        u_own = jnp.concatenate(
            [
                jnp.sum(pr1[0:4, :, 512:].astype(F32), axis=0),
                jnp.sum(pr1[4:8, :, 512:].astype(F32), axis=0),
            ],
            axis=1,
        )
        squares = jnp.sum(u_own * u_own, axis=1, keepdims=True)
        high = squares.astype(BF).astype(F32)
        ys[:, :512] = partial[0].astype(BF)
        ys[:, 512:1024] = partial[1].astype(BF)
        ys[:, 1024:] = jnp.where(lanes((8, 128)) < 64, high, squares - high).astype(BF)
        for dy in (2, 1, 3):
            send(ys, yr.at[y], ys_s, yr_s, at(0, dy, 0, 1))
        yr[y] = ys[...]

        back, ahead = lax.rem(z + 6, 8), lax.rem(z + 2, 8)
        drain(down1.at[pl.ds(0, 4)], d1a_rs)
        for b, a in ((back, ahead), (back + 8, ahead + 8)):
            send(down1.at[b, pl.ds(0, 16)], down1.at[b, pl.ds(0, 16)], d1b_ss, d1b_rs, at(2, 0, 0, 1))
            send(down1.at[a, pl.ds(16, 16)], down1.at[a, pl.ds(16, 16)], d1b_ss, d1b_rs, at(6, 0, 0, 1))
            send(down1.at[b], down1.at[b], d1b_ss, d1b_rs, at(1, 0, 0, 1))
            send(down1.at[a], down1.at[a], d1b_ss, d1b_rs, at(7, 0, 0, 1))

        drain(yr.at[pl.ds(0, 3)], yr_s)
        preact = jnp.sum(yr[...].astype(F32), axis=0)
        squares = jnp.sum(preact[:, 1024:], axis=1, keepdims=True) / 64
        factor = lax.rsqrt(squares / D + EPS)
        act = jnp.square(jnp.maximum(preact[:, :1024] * factor, 0.0)).astype(BF)

        drain(up2.at[pl.ds(0, 2)], u2a_rs)
        send(up2.at[back, pl.ds(0, 2)], up2.at[back, pl.ds(0, 2)], u2b_ss, u2b_rs, at(2, 0, 0, 1))
        send(up2.at[ahead, pl.ds(2, 2)], up2.at[ahead, pl.ds(2, 2)], u2b_ss, u2b_rs, at(6, 0, 0, 1))
        send(up2.at[back], up2.at[back], u2b_ss, u2b_rs, at(1, 0, 0, 1))
        send(up2.at[ahead], up2.at[ahead], u2b_ss, u2b_rs, at(7, 0, 0, 1))

        drain(down1.at[pl.ds(0, 5)], d1c_rs)
        drain(down1.at[pl.ds(0, 6)], d1b_rs)
        branch = nt(act[:, :512], down1[:8].reshape(256, 512)) + nt(act[:, 512:], down1[8:].reshape(256, 512))
        share = jnp.where(x == 0, RESIDUAL, 0.0)
        xs[...] = (branch + share * u_own).astype(BF)
        for dy in (2, 1, 3, 0):
            for dx in (2, 1, 3, 0):
                if dy or dx:
                    send(xs, xr.at[4 * y + x], xs_s, xr_s, at(0, dy, dx, 1))
        xr[4 * y + x] = xs[...]
        loads[6].wait()
        prepare_down2()
        drain(down2.at[0], give_rs)

        drain(xr.at[pl.ds(0, 15)], xr_s)
        middle = jnp.sum(xr[...].astype(F32).reshape(4, 4, 8, 256), axis=1).astype(BF).astype(F32)
        middle = jnp.concatenate([middle[k] for k in range(4)], axis=1)
        squares = jnp.sum(middle * middle, axis=1, keepdims=True)
        factor = lax.rsqrt(squares / D + EPS)
        middle = middle.astype(BF)
        drain(up2.at[pl.ds(0, 2)], u2c_rs)
        drain(up2.at[pl.ds(0, 3)], u2b_rs)
        pre = []
        for k in range(2):
            rows = jnp.concatenate([up2[a, b, k] for b in range(4) for a in range(8)], axis=0)
            pre.append(nn(middle, rows))
        act = jnp.square(jnp.maximum(jnp.concatenate(pre, axis=1) * factor, 0.0))
        acts[...] = act.astype(BF)

        for k in range(32):
            @pl.when(ra != k)
            def _():
                send(acts, actr.at[8 * y + z], as_s, ar_s, {"ra": k, "cb": cb})

        actr[8 * y + z] = acts[...]
        own = jnp.sum(xr[pl.ds(4 * y, 4)].astype(F32), axis=0).astype(BF)
        ms[0] = own[:, :128]
        ms[1] = own[:, 128:]
        for dz in far:
            send(ms.at[lax.div(lax.rem(z + dz, 8), 4)], mr.at[z], ms_s, mr_s, at(dz, 0, 0, 1))
        mr[z] = ms[lax.div(z, 4)]
        drain(mr.at[pl.ds(0, 7)], mr_s)
        mid = mr[...].astype(F32).reshape(64, 128).astype(BF)
        mid = jnp.concatenate([mid, mid], axis=0)
        rs[...] = RESIDUAL * packed_of(nt(place, mid))
        send(rs, rr, rs_s, rr_s, at(0, 0, 0, 0))
        rr[...] = rs[...]

        drain(actr.at[pl.ds(0, 31)], ar_s)
        weights = jnp.concatenate(
            [down2[k, :, 128 * b : 128 * b + 128] for b in range(4) for k in range(2)], axis=1
        )
        gathered = actr[...].astype(F32).reshape(4, 64, 256)
        gathered = jnp.concatenate([gathered[b] for b in range(4)], axis=1).astype(BF)
        gathered = jnp.concatenate([gathered, gathered], axis=0)
        fs[...] = packed_of(nt(weights, gathered)).astype(BF)
        for k in range(4):
            @pl.when(x != k)
            def _():
                send(fs, fr.at[x], fs_s, fr_s, {"ra": ra, "cb": 2 * k + 1})
        for k in range(4):
            send(fs, fr.at[x], fs_s, fr_s, {"ra": ra, "cb": 2 * k})
        fr[x] = fs[...]
        drain(fr.at[pl.ds(0, 3)], fr_s)
        finish()

        drain(pr1.at[pl.ds(0, 7)], ps_s)
        drain(down1.at[pl.ds(0, 2)], d1a_ss)
        drain(down1.at[pl.ds(0, 2)], d1c_ss)
        drain(down1.at[pl.ds(0, 6)], d1b_ss)
        drain(up2s.at[pl.ds(0, 3)], u1_ss)
        drain(yr.at[pl.ds(0, 3)], ys_s)
        drain(up2.at[pl.ds(0, 2)], u2a_ss)
        drain(up2.at[pl.ds(0, 2)], u2c_ss)
        drain(up2.at[pl.ds(0, 3)], u2b_ss)
        drain(xr.at[pl.ds(0, 15)], xs_s)
        drain(actr.at[pl.ds(0, 31)], as_s)
        drain(mr.at[pl.ds(0, 7)], ms_s)
        drain(rr, rs_s)
        drain(xr.at[pl.ds(0, 7)], fs_s)


def local(stream, gain_first, up_first, down_first, gain_second, up_second, down_second):
    vmem = [
        ((32, 64), BF), ((2, 1, 32), F32), ((2, 32, 512), F32), ((2, 32, 512), F32),
        ((32, 512), BF), ((4, 32, 128), BF), ((2, 32, 512), BF),
        ((8, 8, 640), BF), ((8, 8, 512), BF), ((8, 8, 640), BF), ((8, 1152), BF), ((4, 8, 1152), BF),
        ((16, 32, 512), BF), ((4, 2, 32, 128), BF), ((8, 4, 2, 32, 128), BF),
        ((8, 256), BF), ((16, 8, 256), BF), ((2, 8, 128), BF), ((8, 8, 128), BF),
        ((8, 256), BF), ((32, 8, 256), BF), ((16, 128), BF), ((4, 16, 128), BF),
        ((16, 128), F32), ((16, 128), F32),
    ]
    dma = pltpu.SemaphoreType.DMA
    call = pl.pallas_call(
        kernel,
        out_shape=jax.ShapeDtypeStruct((32, 64), BF),
        in_specs=[pl.BlockSpec(memory_space=pl.ANY)] * 7,
        out_specs=pl.BlockSpec(memory_space=pltpu.VMEM),
        scratch_shapes=[pltpu.VMEM(*v) for v in vmem] + [dma((7,))] + [dma(())] * 31
        + [pltpu.SemaphoreType.REGULAR],
        compiler_params=pltpu.CompilerParams(collective_id=0, has_side_effects=True),
    )
    out = call(
        stream.T, gain_first[None], up_first, down_first.T, gain_second[None], up_second, down_second.T
    )
    return out.T


def solution(mesh):
    in_specs = (P(None, "ra"), P("ra"), P("ra", "cb"), P("cb", "ra"), P("ra"), P("ra", "cb"), P("cb", "ra"))
    return jax.shard_map(local, mesh=mesh, in_specs=in_specs, out_specs=P(None, "ra"), check_vma=False)
```

```python
import jax
import jax.numpy as jnp
from jax import lax
from jax.experimental import pallas as pl
from jax.experimental.pallas import tpu as pltpu
from jax.sharding import PartitionSpec as P

D = 1024
EPS = 1e-06
RESIDUAL = 0.25
BF = jnp.bfloat16
F32 = jnp.float32


def nt(a, b):
    return lax.dot_general(a, b, (((1,), (1,)), ((), ())), preferred_element_type=F32)


def nn(a, b):
    return jnp.dot(a, b, preferred_element_type=F32)


def lanes(shape):
    return lax.broadcasted_iota(jnp.int32, shape, len(shape) - 1)


def packed_of(both):
    return jnp.where(lanes((16, 128)) < 64, both[:16], both[16:])


def kernel(
    stream_h, gain_a, up_a, down_a, gain_b, up_b, down_b, out_ref,
    stream_v, gain_v, up_v, down_v,
    down1s, up2s, down2,
    ps, pr0, pr1, ys, yr, down1, up2y, up2, xs, xr, ms, mr, acts, actr, fs, fr, rs, rr,
    load_sem, give_ss, give_rs, ps_s, pr0_s, pr1_s, ys_s, yr_s, d1a_ss, d1a_rs, d1b_ss, d1b_rs,
    u1_ss, u1_rs, u2a_ss, u2a_rs, u2b_ss, u2b_rs,
    xs_s, xr_s, ms_s, mr_s, as_s, ar_s, fs_s, fr_s, rs_s, rr_s, d1c_ss, d1c_rs, u2c_ss, u2c_rs, go,
):
    ra, cb = lax.axis_index("ra"), lax.axis_index("cb")
    z, y = lax.div(ra, 4), lax.rem(ra, 4)
    x, c = lax.div(cb, 2), lax.rem(cb, 2)
    far = (4, 3, 5, 2, 6, 1, 7)
    barrier = pltpu.get_barrier_semaphore()
    loads = [
        pltpu.make_async_copy(src, dst, load_sem.at[k])
        for k, (src, dst) in enumerate(
            [
                (stream_h, stream_v),
                (gain_a, gain_v.at[0]),
                (up_a, up_v.at[0]),
                (down_a, down_v.at[0]),
                (gain_b, gain_v.at[1]),
                (up_b, up_v.at[1]),
                (down_b, down_v.at[1]),
            ]
        )
    ]

    def at(dz, dy, dx, core):
        return {"ra": lax.rem(z + dz, 8) * 4 + lax.rem(y + dy, 4), "cb": lax.rem(x + dx, 4) * 2 + core}

    def send(src, dst, ss, rsem, where):
        pltpu.make_async_remote_copy(
            src_ref=src, dst_ref=dst, send_sem=ss, recv_sem=rsem, device_id=where
        ).start()

    def drain(ref, sem):
        pltpu.make_async_copy(ref, ref, sem).wait()

    def hello(where):
        pl.semaphore_signal(barrier, inc=1, device_id=where)

    def first_up():
        loads[0].wait()
        loads[1].wait()
        u = stream_v[...].astype(F32).T
        loads[2].wait()
        part = nn((u * gain_v[0]).astype(BF), up_v[0].astype(BF))
        ps[:, :, :512] = part.reshape(8, 8, 512).astype(BF)
        return u

    def prepare_up2():
        eye = lax.broadcasted_iota(jnp.int32, (32, 32), 0) == lanes((32, 32))
        loads[4].wait()
        loads[5].wait()
        column = jnp.sum(jnp.where(eye, gain_v[1], 0.0), axis=1, keepdims=True)
        scaled = (up_v[1].astype(BF).astype(F32) * column).astype(BF)
        for k in range(4):
            up2s[k] = scaled[:, 128 * k : 128 * k + 128]

    def prepare_down1():
        loads[3].wait()
        down1s[...] = down_v[0].astype(BF)

    def prepare_down2():
        down2[c] = down_v[1].astype(BF)

    def finish():
        total = jnp.sum(fr[...].astype(F32), axis=0) + rr[...]
        total = total.astype(BF).astype(F32)
        rolled = pltpu.roll(total, 64, 1)
        out_ref[...] = jnp.concatenate([total, rolled], axis=0)[:, :64].astype(BF)

    for load in loads[:3]:
        load.start()

    @pl.when(c == 0)
    def _():
        for dx in range(4):
            hello(at(0, 0, dx, 1))
        for load in loads[3:]:
            load.start()
        first_up()
        prepare_up2()
        prepare_down1()
        pl.semaphore_wait(barrier, 1)
        pl.semaphore_wait(go, 1)
        for dz in far + (0,):
            send(ps.at[lax.rem(z + dz, 8), :, pl.ds(0, 512)], pr0.at[z], ps_s, pr0_s, at(dz, 0, 0, 1))
        for dy in (2, 1, 3, 0):
            send(up2s.at[lax.rem(y + dy, 4)], up2y.at[y, 0], u1_ss, u1_rs, at(0, dy, 0, 1))
        for dz in (2, 6):
            send(down1s, down1.at[z], d1a_ss, d1a_rs, at(dz, 0, 0, 1))
        for dz in (1, 7, 0):
            send(down1s, down1.at[z], d1c_ss, d1c_rs, at(dz, 0, 0, 1))
        partner = at(0, 0, 0, 1)
        loads[6].wait()
        prepare_down2()
        send(down2.at[0], down2.at[0], give_ss, give_rs, partner)
        drain(pr0, ps_s)
        drain(down1.at[pl.ds(0, 2)], d1a_ss)
        drain(down1.at[pl.ds(0, 3)], d1c_ss)
        drain(up2s, u1_ss)
        drain(down2.at[0], give_ss)
        drain(rr, rr_s)
        drain(fr, fr_s)
        finish()

    @pl.when(c == 1)
    def _():
        for dz in far:
            hello(at(dz, 0, 0, 1))
        for d in (2, 1, 3):
            hello(at(0, d, 0, 1))
            hello(at(0, 0, d, 1))
        hello(at(0, 0, 0, 0))
        for load in loads[3:]:
            load.start()

        u = first_up()
        place = lanes((32, 128)) == 32 * lax.rem(z, 4) + lax.broadcasted_iota(jnp.int32, (32, 128), 0)
        place = place.astype(F32).astype(BF)
        ps[:, :, 512:] = nn(u.astype(BF), place).reshape(8, 8, 128).astype(BF)
        prepare_up2()
        prepare_down1()

        pl.semaphore_wait(barrier, 17)
        pl.semaphore_signal(go, inc=1, device_id=at(0, 0, 0, 0))
        for dz in far:
            send(ps.at[lax.rem(z + dz, 8)], pr1.at[z], ps_s, pr1_s, at(dz, 0, 0, 1))
        for dy in (2, 1, 3):
            send(up2s.at[lax.rem(y + dy, 4)], up2y.at[y, 1], u1_ss, u1_rs, at(0, dy, 0, 1))
        for dz in (2, 6):
            send(down1s, down1.at[8 + z], d1a_ss, d1a_rs, at(dz, 0, 0, 1))
        for dz in (1, 7):
            send(down1s, down1.at[8 + z], d1c_ss, d1c_rs, at(dz, 0, 0, 1))
        pr1[z] = ps[z]
        down1[8 + z] = down1s[...]
        up2y[y, 1] = up2s[y]
        drain(down1.at[pl.ds(0, 7), :, pl.ds(0, 128)], u1_rs)
        for dz in (2, 6):
            send(up2y, up2.at[z], u2a_ss, u2a_rs, at(dz, 0, 0, 1))
        for dz in (1, 7):
            send(up2y, up2.at[z], u2c_ss, u2c_rs, at(dz, 0, 0, 1))
        up2[z] = up2y[...]

        drain(pr0, pr0_s)
        drain(pr1.at[pl.ds(0, 7)], pr1_s)
        partial = [jnp.sum(pr0[...].astype(F32), axis=0), jnp.sum(pr1[:, :, :512].astype(F32), axis=0)]
        u_own = jnp.concatenate(
            [
                jnp.sum(pr1[0:4, :, 512:].astype(F32), axis=0),
                jnp.sum(pr1[4:8, :, 512:].astype(F32), axis=0),
            ],
            axis=1,
        )
        squares = jnp.sum(u_own * u_own, axis=1, keepdims=True)
        high = squares.astype(BF).astype(F32)
        ys[:, :512] = partial[0].astype(BF)
        ys[:, 512:1024] = partial[1].astype(BF)
        ys[:, 1024:] = jnp.where(lanes((8, 128)) < 64, high, squares - high).astype(BF)
        for dy in (2, 1, 3):
            send(ys, yr.at[y], ys_s, yr_s, at(0, dy, 0, 1))
        yr[y] = ys[...]

        back, ahead = lax.rem(z + 6, 8), lax.rem(z + 2, 8)
        drain(down1.at[pl.ds(0, 4)], d1a_rs)
        for b, a in ((back, ahead), (back + 8, ahead + 8)):
            send(down1.at[b, pl.ds(0, 16)], down1.at[b, pl.ds(0, 16)], d1b_ss, d1b_rs, at(2, 0, 0, 1))
            send(down1.at[a, pl.ds(16, 16)], down1.at[a, pl.ds(16, 16)], d1b_ss, d1b_rs, at(6, 0, 0, 1))
            send(down1.at[b], down1.at[b], d1b_ss, d1b_rs, at(1, 0, 0, 1))
            send(down1.at[a], down1.at[a], d1b_ss, d1b_rs, at(7, 0, 0, 1))

        drain(yr.at[pl.ds(0, 3)], yr_s)
        preact = jnp.sum(yr[...].astype(F32), axis=0)
        squares = jnp.sum(preact[:, 1024:], axis=1, keepdims=True) / 64
        factor = lax.rsqrt(squares / D + EPS)
        act = jnp.square(jnp.maximum(preact[:, :1024] * factor, 0.0)).astype(BF)

        drain(up2.at[pl.ds(0, 2)], u2a_rs)
        send(up2.at[back, pl.ds(0, 2)], up2.at[back, pl.ds(0, 2)], u2b_ss, u2b_rs, at(2, 0, 0, 1))
        send(up2.at[ahead, pl.ds(2, 2)], up2.at[ahead, pl.ds(2, 2)], u2b_ss, u2b_rs, at(6, 0, 0, 1))
        send(up2.at[back], up2.at[back], u2b_ss, u2b_rs, at(1, 0, 0, 1))
        send(up2.at[ahead], up2.at[ahead], u2b_ss, u2b_rs, at(7, 0, 0, 1))

        drain(down1.at[pl.ds(0, 5)], d1c_rs)
        drain(down1.at[pl.ds(0, 6)], d1b_rs)
        branch = nt(act[:, :512], down1[:8].reshape(256, 512)) + nt(act[:, 512:], down1[8:].reshape(256, 512))
        share = jnp.where(x == 0, RESIDUAL, 0.0)
        xs[...] = (branch + share * u_own).astype(BF)
        for dy in (2, 1, 3, 0):
            for dx in (2, 1, 3, 0):
                if dy or dx:
                    send(xs, xr.at[4 * y + x], xs_s, xr_s, at(0, dy, dx, 1))
        xr[4 * y + x] = xs[...]
        loads[6].wait()
        prepare_down2()
        drain(down2.at[0], give_rs)

        drain(xr.at[pl.ds(0, 15)], xr_s)
        middle = jnp.sum(xr[...].astype(F32).reshape(4, 4, 8, 256), axis=1).astype(BF).astype(F32)
        middle = jnp.concatenate([middle[k] for k in range(4)], axis=1)
        squares = jnp.sum(middle * middle, axis=1, keepdims=True)
        factor = lax.rsqrt(squares / D + EPS)
        middle = middle.astype(BF)
        drain(up2.at[pl.ds(0, 2)], u2c_rs)
        drain(up2.at[pl.ds(0, 3)], u2b_rs)
        pre = []
        for k in range(2):
            rows = jnp.concatenate([up2[a, b, k] for b in range(4) for a in range(8)], axis=0)
            pre.append(nn(middle, rows))
        act = jnp.square(jnp.maximum(jnp.concatenate(pre, axis=1) * factor, 0.0))
        acts[...] = act.astype(BF)

        for k in range(32):
            @pl.when(ra != k)
            def _():
                send(acts, actr.at[8 * y + z], as_s, ar_s, {"ra": k, "cb": cb})

        actr[8 * y + z] = acts[...]
        own = jnp.sum(xr[pl.ds(4 * y, 4)].astype(F32), axis=0).astype(BF)
        ms[0] = own[:, :128]
        ms[1] = own[:, 128:]
        for dz in far:
            send(ms.at[lax.div(lax.rem(z + dz, 8), 4)], mr.at[z], ms_s, mr_s, at(dz, 0, 0, 1))
        mr[z] = ms[lax.div(z, 4)]
        drain(mr.at[pl.ds(0, 7)], mr_s)
        mid = mr[...].astype(F32).reshape(64, 128).astype(BF)
        mid = jnp.concatenate([mid, mid], axis=0)
        rs[...] = RESIDUAL * packed_of(nt(place, mid))
        send(rs, rr, rs_s, rr_s, at(0, 0, 0, 0))
        rr[...] = rs[...]

        drain(actr.at[pl.ds(0, 31)], ar_s)
        weights = jnp.concatenate(
            [down2[k, :, 128 * b : 128 * b + 128] for b in range(4) for k in range(2)], axis=1
        )
        gathered = actr[...].astype(F32).reshape(4, 64, 256)
        gathered = jnp.concatenate([gathered[b] for b in range(4)], axis=1).astype(BF)
        gathered = jnp.concatenate([gathered, gathered], axis=0)
        fs[...] = packed_of(nt(weights, gathered)).astype(BF)
        for k in range(4):
            @pl.when(x != k)
            def _():
                send(fs, fr.at[x], fs_s, fr_s, {"ra": ra, "cb": 2 * k + 1})
        for k in range(4):
            send(fs, fr.at[x], fs_s, fr_s, {"ra": ra, "cb": 2 * k})
        fr[x] = fs[...]
        drain(fr.at[pl.ds(0, 3)], fr_s)
        finish()

        drain(pr1.at[pl.ds(0, 7)], ps_s)
        drain(down1.at[pl.ds(0, 2)], d1a_ss)
        drain(down1.at[pl.ds(0, 2)], d1c_ss)
        drain(down1.at[pl.ds(0, 6)], d1b_ss)
        drain(up2s.at[pl.ds(0, 3)], u1_ss)
        drain(yr.at[pl.ds(0, 3)], ys_s)
        drain(up2.at[pl.ds(0, 2)], u2a_ss)
        drain(up2.at[pl.ds(0, 2)], u2c_ss)
        drain(up2.at[pl.ds(0, 3)], u2b_ss)
        drain(xr.at[pl.ds(0, 15)], xs_s)
        drain(actr.at[pl.ds(0, 31)], as_s)
        drain(mr.at[pl.ds(0, 7)], ms_s)
        drain(rr, rs_s)
        drain(xr.at[pl.ds(0, 7)], fs_s)


def local(stream, gain_first, up_first, down_first, gain_second, up_second, down_second):
    vmem = [
        ((32, 64), BF), ((2, 1, 32), F32), ((2, 32, 512), F32), ((2, 32, 512), F32),
        ((32, 512), BF), ((4, 32, 128), BF), ((2, 32, 512), BF),
        ((8, 8, 640), BF), ((8, 8, 512), BF), ((8, 8, 640), BF), ((8, 1152), BF), ((4, 8, 1152), BF),
        ((16, 32, 512), BF), ((4, 2, 32, 128), BF), ((8, 4, 2, 32, 128), BF),
        ((8, 256), BF), ((16, 8, 256), BF), ((2, 8, 128), BF), ((8, 8, 128), BF),
        ((8, 256), BF), ((32, 8, 256), BF), ((16, 128), BF), ((4, 16, 128), BF),
        ((16, 128), F32), ((16, 128), F32),
    ]
    dma = pltpu.SemaphoreType.DMA
    call = pl.pallas_call(
        kernel,
        out_shape=jax.ShapeDtypeStruct((32, 64), BF),
        in_specs=[pl.BlockSpec(memory_space=pl.ANY)] * 7,
        out_specs=pl.BlockSpec(memory_space=pltpu.VMEM),
        scratch_shapes=[pltpu.VMEM(*v) for v in vmem] + [dma((7,))] + [dma(())] * 31
        + [pltpu.SemaphoreType.REGULAR],
        compiler_params=pltpu.CompilerParams(collective_id=0, has_side_effects=True, vmem_limit_bytes=56535040),
    )
    out = call(
        stream.T, gain_first[None], up_first, down_first.T, gain_second[None], up_second, down_second.T
    )
    return out.T


def solution(mesh):
    in_specs = (P(None, "ra"), P("ra"), P("ra", "cb"), P("cb", "ra"), P("ra"), P("ra", "cb"), P("cb", "ra"))
    return jax.shard_map(local, mesh=mesh, in_specs=in_specs, out_specs=P(None, "ra"), check_vma=False)
```

```python
import jax
import jax.numpy as jnp
from jax import lax
from jax.experimental import pallas as pl
from jax.experimental.pallas import tpu as pltpu
from jax.sharding import PartitionSpec as P

D = 1024
EPS = 1e-06
RESIDUAL = 0.25
BF = jnp.bfloat16
F32 = jnp.float32


def nt(a, b):
    return lax.dot_general(a, b, (((1,), (1,)), ((), ())), preferred_element_type=F32)


def nn(a, b):
    return jnp.dot(a, b, preferred_element_type=F32)


def lanes(shape):
    return lax.broadcasted_iota(jnp.int32, shape, len(shape) - 1)


def kernel(
    stream_h, gain_a, up_a, down_a, gain_b, up_b, down_b, out_ref,
    stream_v, gain_v, up_v, down_v,
    down1s, up2s, down2,
    ps, pr0, pr1, ys, yr, down1, up2y, up2, xs, xr, ms, mr, acts, actr, fs, fr, rs, rr,
    load_sem, fs_s, d1a_rs, give_ss, give_rs, ps_s, pr0_s, pr1_s, ys_s, yr_s, d1a_ss, d1b_ss, d1b_rs,
    u1_ss, u1_rs, u2a_ss, u2a_rs, u2b_ss, u2b_rs,
    xs_s, xr_s, ms_s, mr_s, as_s, ar_s, fr_s, rs_s, rr_s, d1c_ss, d1c_rs, u2c_ss, u2c_rs, go,
):
    ra, cb = lax.axis_index("ra"), lax.axis_index("cb")
    z, y = lax.div(ra, 4), lax.rem(ra, 4)
    x, c = lax.div(cb, 2), lax.rem(cb, 2)
    far = (4, 3, 5, 2, 6, 1, 7)
    barrier = pltpu.get_barrier_semaphore()
    loads = [
        pltpu.make_async_copy(src, dst, load_sem.at[k])
        for k, (src, dst) in enumerate(
            [
                (stream_h, stream_v),
                (gain_a, gain_v.at[0]),
                (up_a, up_v.at[0]),
                (down_a, down_v.at[0]),
                (gain_b, gain_v.at[1]),
                (up_b, up_v.at[1]),
                (down_b, down_v.at[1]),
            ]
        )
    ]

    def at(dz, dy, dx, core):
        return {"ra": lax.rem(z + dz, 8) * 4 + lax.rem(y + dy, 4), "cb": lax.rem(x + dx, 4) * 2 + core}

    def send(src, dst, ss, rsem, where):
        pltpu.make_async_remote_copy(
            src_ref=src, dst_ref=dst, send_sem=ss, recv_sem=rsem, device_id=where
        ).start()

    def drain(ref, sem):
        pltpu.make_async_copy(ref, ref, sem).wait()

    def hello(where):
        pl.semaphore_signal(barrier, inc=1, device_id=where)

    def first_up():
        loads[0].wait()
        loads[1].wait()
        u = stream_v[...].astype(F32).T
        loads[2].wait()
        part = nn((u * gain_v[0]).astype(BF), up_v[0].astype(BF))
        ps[:, :, :512] = part.reshape(8, 8, 512).astype(BF)
        return u

    def prepare_up2():
        eye = lax.broadcasted_iota(jnp.int32, (32, 32), 0) == lanes((32, 32))
        loads[4].wait()
        loads[5].wait()
        column = jnp.sum(jnp.where(eye, gain_v[1], 0.0), axis=1, keepdims=True)
        scaled = (up_v[1].astype(BF).astype(F32) * column).astype(BF)
        for k in range(4):
            up2s[k] = scaled[:, 128 * k : 128 * k + 128]

    def prepare_down1():
        loads[3].wait()
        down1s[...] = down_v[0].astype(BF)

    def prepare_down2():
        down2[c] = down_v[1].astype(BF)

    def finish():
        out_ref[...] = (jnp.sum(fr[...].astype(F32), axis=0) + rr[...]).astype(BF)

    @pl.when(c == 0)
    def _():
        for load in loads[:3]:
            load.start()
        for dx in range(4):
            hello(at(0, 0, dx, 1))
        for load in loads[3:]:
            load.start()
        first_up()
        prepare_up2()
        prepare_down1()
        pl.semaphore_wait(barrier, 1)
        pl.semaphore_wait(go, 1)
        for dz in far + (0,):
            send(ps.at[lax.rem(z + dz, 8), :, pl.ds(0, 512)], pr0.at[z], ps_s, pr0_s, at(dz, 0, 0, 1))
        for dy in (2, 1, 3, 0):
            send(up2s.at[lax.rem(y + dy, 4)], up2y.at[y, 0], u1_ss, u1_rs, at(0, dy, 0, 1))
        for dz in (2, 6):
            send(down1s, down1.at[z], d1a_ss, d1a_rs.at[0], at(dz, 0, 0, 1))
        for dz in (1, 7, 0):
            send(down1s, down1.at[z], d1c_ss, d1c_rs, at(dz, 0, 0, 1))
        partner = at(0, 0, 0, 1)
        loads[6].wait()
        prepare_down2()
        send(down2.at[0], down2.at[0], give_ss, give_rs, partner)
        drain(pr0, ps_s)
        drain(down1.at[pl.ds(0, 2)], d1a_ss)
        drain(down1.at[pl.ds(0, 3)], d1c_ss)
        drain(up2s, u1_ss)
        drain(down2.at[0], give_ss)
        drain(rr, rr_s)
        drain(fr, fr_s)
        finish()

    @pl.when(c == 1)
    def _():
        for dz in far:
            hello(at(dz, 0, 0, 1))
        for load in loads[:3]:
            load.start()
        for d in (2, 1, 3):
            hello(at(0, d, 0, 1))
            hello(at(0, 0, d, 1))
        hello(at(0, 0, 0, 0))
        for load in loads[3:]:
            load.start()

        u = first_up()
        place = lanes((32, 128)) == 32 * lax.rem(z, 4) + lax.broadcasted_iota(jnp.int32, (32, 128), 0)
        place = place.astype(F32).astype(BF)
        ps[:, :, 512:] = nn(u.astype(BF), place).reshape(8, 8, 128).astype(BF)
        prepare_up2()
        prepare_down1()

        pl.semaphore_wait(barrier, 17)
        pl.semaphore_signal(go, inc=1, device_id=at(0, 0, 0, 0))
        for dz in far:
            send(ps.at[lax.rem(z + dz, 8)], pr1.at[z], ps_s, pr1_s, at(dz, 0, 0, 1))
        for dy in (2, 1, 3):
            send(up2s.at[lax.rem(y + dy, 4)], up2y.at[y, 1], u1_ss, u1_rs, at(0, dy, 0, 1))
        for dz in (2, 6):
            send(down1s, down1.at[8 + z], d1a_ss, d1a_rs.at[1], at(dz, 0, 0, 1))
        for dz in (1, 7):
            send(down1s, down1.at[8 + z], d1c_ss, d1c_rs, at(dz, 0, 0, 1))
        pr1[z] = ps[z]
        down1[8 + z] = down1s[...]
        up2y[y, 1] = up2s[y]
        drain(down1.at[pl.ds(0, 7), :, pl.ds(0, 128)], u1_rs)
        for dz in (2, 6):
            send(up2y, up2.at[z], u2a_ss, u2a_rs, at(dz, 0, 0, 1))
        up2[z] = up2y[...]
        back, ahead = lax.rem(z + 6, 8), lax.rem(z + 2, 8)
        drain(down1.at[pl.ds(0, 2)], d1a_rs.at[1])
        b, a = back + 8, ahead + 8
        send(down1.at[b, pl.ds(0, 16)], down1.at[b, pl.ds(0, 16)], d1b_ss, d1b_rs, at(2, 0, 0, 1))
        send(down1.at[a, pl.ds(16, 16)], down1.at[a, pl.ds(16, 16)], d1b_ss, d1b_rs, at(6, 0, 0, 1))
        send(down1.at[b], down1.at[b], d1b_ss, d1b_rs, at(1, 0, 0, 1))
        send(down1.at[a], down1.at[a], d1b_ss, d1b_rs, at(7, 0, 0, 1))


        drain(pr0, pr0_s)
        drain(pr1.at[pl.ds(0, 7)], pr1_s)
        partial = [jnp.sum(pr0[...].astype(F32), axis=0), jnp.sum(pr1[:, :, :512].astype(F32), axis=0)]
        u_own = jnp.concatenate(
            [
                jnp.sum(pr1[0:4, :, 512:].astype(F32), axis=0),
                jnp.sum(pr1[4:8, :, 512:].astype(F32), axis=0),
            ],
            axis=1,
        )
        squares = jnp.sum(u_own * u_own, axis=1, keepdims=True)
        high = squares.astype(BF).astype(F32)
        ys[:, :512] = partial[0].astype(BF)
        ys[:, 512:1024] = partial[1].astype(BF)
        ys[:, 1024:] = jnp.where(lanes((8, 128)) < 64, high, squares - high).astype(BF)
        for dy in (2, 1, 3):
            send(ys, yr.at[y], ys_s, yr_s, at(0, dy, 0, 1))
        yr[y] = ys[...]

        drain(down1.at[pl.ds(0, 2)], d1a_rs.at[0])
        b, a = back + 0, ahead + 0
        send(down1.at[b, pl.ds(0, 16)], down1.at[b, pl.ds(0, 16)], d1b_ss, d1b_rs, at(2, 0, 0, 1))
        send(down1.at[a, pl.ds(16, 16)], down1.at[a, pl.ds(16, 16)], d1b_ss, d1b_rs, at(6, 0, 0, 1))
        send(down1.at[b], down1.at[b], d1b_ss, d1b_rs, at(1, 0, 0, 1))
        send(down1.at[a], down1.at[a], d1b_ss, d1b_rs, at(7, 0, 0, 1))

        for dz in (1, 7):
            send(up2y, up2.at[z], u2c_ss, u2c_rs, at(dz, 0, 0, 1))
        drain(yr.at[pl.ds(0, 3)], yr_s)
        preact = jnp.sum(yr[...].astype(F32), axis=0)
        squares = jnp.sum(preact[:, 1024:], axis=1, keepdims=True) / 64
        factor = lax.rsqrt(squares / D + EPS)
        act = jnp.square(jnp.maximum(preact[:, :1024] * factor, 0.0)).astype(BF)

        drain(up2.at[pl.ds(0, 2)], u2a_rs)
        send(up2.at[back, pl.ds(0, 2)], up2.at[back, pl.ds(0, 2)], u2b_ss, u2b_rs, at(2, 0, 0, 1))
        send(up2.at[ahead, pl.ds(2, 2)], up2.at[ahead, pl.ds(2, 2)], u2b_ss, u2b_rs, at(6, 0, 0, 1))
        send(up2.at[back], up2.at[back], u2b_ss, u2b_rs, at(1, 0, 0, 1))
        send(up2.at[ahead], up2.at[ahead], u2b_ss, u2b_rs, at(7, 0, 0, 1))

        drain(down1.at[pl.ds(0, 5)], d1c_rs)
        drain(down1.at[pl.ds(0, 6)], d1b_rs)
        branch = nt(act[:, :512], down1[:8].reshape(256, 512)) + nt(act[:, 512:], down1[8:].reshape(256, 512))
        share = jnp.where(x == 0, RESIDUAL, 0.0)
        xs[...] = (branch + share * u_own).astype(BF)
        for dy in (2, 1, 3, 0):
            for dx in (2, 1, 3, 0):
                if dy or dx:
                    send(xs, xr.at[4 * y + x], xs_s, xr_s, at(0, dy, dx, 1))
        xr[4 * y + x] = xs[...]
        loads[6].wait()
        prepare_down2()
        drain(down2.at[0], give_rs)

        drain(xr.at[pl.ds(0, 15)], xr_s)
        middle = jnp.sum(xr[...].astype(F32).reshape(4, 4, 8, 256), axis=1).astype(BF).astype(F32)
        middle = jnp.concatenate([middle[k] for k in range(4)], axis=1)
        squares = jnp.sum(middle * middle, axis=1, keepdims=True)
        factor = lax.rsqrt(squares / D + EPS)
        middle = middle.astype(BF)
        drain(up2.at[pl.ds(0, 2)], u2c_rs)
        drain(up2.at[pl.ds(0, 3)], u2b_rs)
        pre = []
        for k in range(2):
            rows = jnp.concatenate([up2[a, b, k] for b in range(4) for a in range(8)], axis=0)
            pre.append(nn(middle, rows))
        act = jnp.square(jnp.maximum(jnp.concatenate(pre, axis=1) * factor, 0.0))
        acts[...] = act.astype(BF)

        for k in range(32):
            @pl.when(ra != k)
            def _():
                send(acts, actr.at[8 * y + z], as_s, ar_s, {"ra": k, "cb": cb})

        actr[8 * y + z] = acts[...]
        own = jnp.sum(xr[pl.ds(4 * y, 4)].astype(F32), axis=0).astype(BF)
        ms[0] = own[:, :128]
        ms[1] = own[:, 128:]
        for dz in far:
            send(ms.at[lax.div(lax.rem(z + dz, 8), 4)], mr.at[z], ms_s, mr_s, at(dz, 0, 0, 1))
        mr[z] = ms[lax.div(z, 4)]

        drain(actr.at[pl.ds(0, 31)], ar_s)
        weights = jnp.concatenate(
            [down2[k, :, 128 * b : 128 * b + 128] for b in range(4) for k in range(2)], axis=1
        )
        gathered = actr[...].astype(F32).reshape(4, 64, 256)
        gathered = jnp.concatenate([gathered[b] for b in range(4)], axis=1).astype(BF)
        fs[...] = nt(weights, gathered).astype(BF)
        for k in range(4):
            @pl.when(x != k)
            def _():
                send(fs, fr.at[x], fs_s.at[1], fr_s, {"ra": ra, "cb": 2 * k + 1})
        for k in range(4):
            send(fs, fr.at[x], fs_s.at[0], fr_s, {"ra": ra, "cb": 2 * k})
        fr[x] = fs[...]
        drain(mr.at[pl.ds(0, 7)], mr_s)
        mid = mr[...].astype(F32).reshape(64, 128).astype(BF)
        rs[...] = RESIDUAL * nt(place, mid)
        send(rs, rr, rs_s, rr_s, at(0, 0, 0, 0))
        rr[...] = rs[...]
        drain(fr.at[pl.ds(0, 3)], fr_s)
        finish()

        drain(pr1.at[pl.ds(0, 7)], ps_s)
        drain(down1.at[pl.ds(0, 2)], d1a_ss)
        drain(down1.at[pl.ds(0, 2)], d1c_ss)
        drain(down1.at[pl.ds(0, 6)], d1b_ss)
        drain(up2s.at[pl.ds(0, 3)], u1_ss)
        drain(yr.at[pl.ds(0, 3)], ys_s)
        drain(up2.at[pl.ds(0, 2)], u2a_ss)
        drain(up2.at[pl.ds(0, 2)], u2c_ss)
        drain(up2.at[pl.ds(0, 3)], u2b_ss)
        drain(xr.at[pl.ds(0, 15)], xs_s)
        drain(actr.at[pl.ds(0, 31)], as_s)
        drain(mr.at[pl.ds(0, 7)], ms_s)
        drain(rr, rs_s)
        drain(fr, fs_s.at[0])
        drain(fr.at[pl.ds(0, 3)], fs_s.at[1])


def local(stream, gain_first, up_first, down_first, gain_second, up_second, down_second):
    vmem = [
        ((32, 64), BF), ((2, 1, 32), F32), ((2, 32, 512), F32), ((2, 32, 512), F32),
        ((32, 512), BF), ((4, 32, 128), BF), ((2, 32, 512), BF),
        ((8, 8, 640), BF), ((8, 8, 512), BF), ((8, 8, 640), BF), ((8, 1152), BF), ((4, 8, 1152), BF),
        ((16, 32, 512), BF), ((4, 2, 32, 128), BF), ((8, 4, 2, 32, 128), BF),
        ((8, 256), BF), ((16, 8, 256), BF), ((2, 8, 128), BF), ((8, 8, 128), BF),
        ((8, 256), BF), ((32, 8, 256), BF), ((32, 64), BF), ((4, 32, 64), BF),
        ((32, 64), F32), ((32, 64), F32),
    ]
    dma = pltpu.SemaphoreType.DMA
    call = pl.pallas_call(
        kernel,
        out_shape=jax.ShapeDtypeStruct((32, 64), BF),
        in_specs=[pl.BlockSpec(memory_space=pl.ANY)] * 7,
        out_specs=pl.BlockSpec(memory_space=pltpu.VMEM),
        scratch_shapes=[pltpu.VMEM(*v) for v in vmem] + [dma((7,)), dma((2,)), dma((2,))] + [dma(())] * 29
        + [pltpu.SemaphoreType.REGULAR],
        compiler_params=pltpu.CompilerParams(collective_id=0, has_side_effects=True, vmem_limit_bytes=56535040),
    )
    out = call(
        stream.T, gain_first[None], up_first, down_first.T, gain_second[None], up_second, down_second.T
    )
    return out.T


def solution(mesh):
    in_specs = (P(None, "ra"), P("ra"), P("ra", "cb"), P("cb", "ra"), P("ra"), P("ra", "cb"), P("cb", "ra"))
    return jax.shard_map(local, mesh=mesh, in_specs=in_specs, out_specs=P(None, "ra"), check_vma=False)
```

```python
import jax
import jax.numpy as jnp
from jax import lax
from jax.experimental import pallas as pl
from jax.experimental.pallas import tpu as pltpu
from jax.sharding import PartitionSpec as P

D = 1024
EPS = 1e-06
RESIDUAL = 0.25
BF = jnp.bfloat16
F32 = jnp.float32


def nt(a, b):
    return lax.dot_general(a, b, (((1,), (1,)), ((), ())), preferred_element_type=F32)


def nn(a, b):
    return jnp.dot(a, b, preferred_element_type=F32)


def lanes(shape):
    return lax.broadcasted_iota(jnp.int32, shape, len(shape) - 1)


def kernel(
    stream_h, gain_a, up_a, down_a, gain_b, up_b, down_b, out_ref,
    stream_v, gain_v, up_v, down_v,
    down1s, up2s, down2,
    ps, pr0, pr1, ys, yr, down1, up2y, up2, xs, xr, ms, mr, acts, actr, fs, fr, rs, rr,
    load_sem, fs_s, d1a_rs, give_ss, give_rs, ps_s, pr0_s, pr1_s, ys_s, yr_s, d1a_ss, d1b_ss, d1b_rs,
    u1_ss, u1_rs, u2a_ss, u2a_rs, u2b_ss, u2b_rs,
    xs_s, xr_s, ms_s, mr_s, as_s, ar_s, fr_s, rs_s, rr_s, d1c_ss, d1c_rs, u2c_ss, u2c_rs, go,
):
    ra, cb = lax.axis_index("ra"), lax.axis_index("cb")
    z, y = lax.div(ra, 4), lax.rem(ra, 4)
    x, c = lax.div(cb, 2), lax.rem(cb, 2)
    far = (4, 3, 5, 2, 6, 1, 7)
    barrier = pltpu.get_barrier_semaphore()
    loads = [
        pltpu.make_async_copy(src, dst, load_sem.at[k])
        for k, (src, dst) in enumerate(
            [
                (stream_h, stream_v),
                (gain_a, gain_v.at[0]),
                (up_a, up_v.at[0]),
                (down_a, down_v.at[0]),
                (gain_b, gain_v.at[1]),
                (up_b, up_v.at[1]),
                (down_b, down_v.at[1]),
            ]
        )
    ]

    def at(dz, dy, dx, core):
        return {"ra": lax.rem(z + dz, 8) * 4 + lax.rem(y + dy, 4), "cb": lax.rem(x + dx, 4) * 2 + core}

    def send(src, dst, ss, rsem, where):
        pltpu.make_async_remote_copy(
            src_ref=src, dst_ref=dst, send_sem=ss, recv_sem=rsem, device_id=where
        ).start()

    def drain(ref, sem):
        pltpu.make_async_copy(ref, ref, sem).wait()

    def hello(where):
        pl.semaphore_signal(barrier, inc=1, device_id=where)

    def first_up():
        loads[0].wait()
        loads[1].wait()
        u = stream_v[...].astype(F32).T
        loads[2].wait()
        part = nn((u * gain_v[0]).astype(BF), up_v[0].astype(BF))
        ps[:, :, :512] = part.reshape(8, 8, 512).astype(BF)
        return u

    def prepare_up2():
        eye = lax.broadcasted_iota(jnp.int32, (32, 32), 0) == lanes((32, 32))
        loads[4].wait()
        loads[5].wait()
        column = jnp.sum(jnp.where(eye, gain_v[1], 0.0), axis=1, keepdims=True)
        scaled = (up_v[1].astype(BF).astype(F32) * column).astype(BF)
        for k in range(4):
            up2s[k] = scaled[:, 128 * k : 128 * k + 128]

    def prepare_down1():
        loads[3].wait()
        down1s[...] = down_v[0].astype(BF)

    def prepare_down2():
        down2[c] = down_v[1].astype(BF)

    def finish():
        out_ref[...] = (jnp.sum(fr[...].astype(F32), axis=0) + rr[...]).astype(BF)

    @pl.when(c == 0)
    def _():
        for load in loads[:3]:
            load.start()
        for dx in range(4):
            hello(at(0, 0, dx, 1))
        for load in loads[3:]:
            load.start()
        first_up()
        prepare_up2()
        prepare_down1()
        pl.semaphore_wait(barrier, 1)
        pl.semaphore_wait(go, 1)
        for dy in (2, 1, 3, 0):
            send(up2s.at[lax.rem(y + dy, 4)], up2y.at[y, 0], u1_ss, u1_rs, at(0, dy, 0, 1))
        for dz in far + (0,):
            send(ps.at[lax.rem(z + dz, 8), :, pl.ds(0, 512)], pr0.at[z], ps_s, pr0_s, at(dz, 0, 0, 1))
        for dz in (2, 6):
            send(down1s, down1.at[z], d1a_ss, d1a_rs.at[0], at(dz, 0, 0, 1))
        for dz in (1, 7, 0):
            send(down1s, down1.at[z], d1c_ss, d1c_rs, at(dz, 0, 0, 1))
        partner = at(0, 0, 0, 1)
        loads[6].wait()
        prepare_down2()
        send(down2.at[0], down2.at[0], give_ss, give_rs, partner)
        drain(pr0, ps_s)
        drain(down1.at[pl.ds(0, 2)], d1a_ss)
        drain(down1.at[pl.ds(0, 3)], d1c_ss)
        drain(up2s, u1_ss)
        drain(down2.at[0], give_ss)
        drain(rr, rr_s)
        drain(fr, fr_s)
        finish()

    @pl.when(c == 1)
    def _():
        for dz in far:
            hello(at(dz, 0, 0, 1))
        for load in loads[:3]:
            load.start()
        for d in (2, 1, 3):
            hello(at(0, d, 0, 1))
            hello(at(0, 0, d, 1))
        hello(at(0, 0, 0, 0))
        for load in loads[3:]:
            load.start()

        u = first_up()
        place = lanes((32, 128)) == 32 * lax.rem(z, 4) + lax.broadcasted_iota(jnp.int32, (32, 128), 0)
        place = place.astype(F32).astype(BF)
        ps[:, :, 512:] = nn(u.astype(BF), place).reshape(8, 8, 128).astype(BF)
        prepare_up2()
        prepare_down1()

        pl.semaphore_wait(barrier, 17)
        pl.semaphore_signal(go, inc=1, device_id=at(0, 0, 0, 0))
        for dy in (2, 1, 3):
            send(up2s.at[lax.rem(y + dy, 4)], up2y.at[y, 1], u1_ss, u1_rs, at(0, dy, 0, 1))
        for dz in (2, 6):
            send(down1s, down1.at[8 + z], d1a_ss, d1a_rs.at[1], at(dz, 0, 0, 1))
        for dz in far:
            send(ps.at[lax.rem(z + dz, 8)], pr1.at[z], ps_s, pr1_s, at(dz, 0, 0, 1))
        for dz in (1, 7):
            send(down1s, down1.at[8 + z], d1c_ss, d1c_rs, at(dz, 0, 0, 1))
        pr1[z] = ps[z]
        down1[8 + z] = down1s[...]
        up2y[y, 1] = up2s[y]
        drain(down1.at[pl.ds(0, 7), :, pl.ds(0, 128)], u1_rs)
        for dz in (2, 6):
            send(up2y, up2.at[z], u2a_ss, u2a_rs, at(dz, 0, 0, 1))
        up2[z] = up2y[...]
        back, ahead = lax.rem(z + 6, 8), lax.rem(z + 2, 8)
        drain(down1.at[pl.ds(0, 2)], d1a_rs.at[1])
        b, a = back + 8, ahead + 8
        send(down1.at[b, pl.ds(0, 16)], down1.at[b, pl.ds(0, 16)], d1b_ss, d1b_rs, at(2, 0, 0, 1))
        send(down1.at[a, pl.ds(16, 16)], down1.at[a, pl.ds(16, 16)], d1b_ss, d1b_rs, at(6, 0, 0, 1))
        send(down1.at[b], down1.at[b], d1b_ss, d1b_rs, at(1, 0, 0, 1))
        send(down1.at[a], down1.at[a], d1b_ss, d1b_rs, at(7, 0, 0, 1))


        drain(pr0, pr0_s)
        drain(pr1.at[pl.ds(0, 7)], pr1_s)
        partial = [jnp.sum(pr0[...].astype(F32), axis=0), jnp.sum(pr1[:, :, :512].astype(F32), axis=0)]
        u_own = jnp.concatenate(
            [
                jnp.sum(pr1[0:4, :, 512:].astype(F32), axis=0),
                jnp.sum(pr1[4:8, :, 512:].astype(F32), axis=0),
            ],
            axis=1,
        )
        squares = jnp.sum(u_own * u_own, axis=1, keepdims=True)
        high = squares.astype(BF).astype(F32)
        ys[:, :512] = partial[0].astype(BF)
        ys[:, 512:1024] = partial[1].astype(BF)
        ys[:, 1024:] = jnp.where(lanes((8, 128)) < 64, high, squares - high).astype(BF)
        for dy in (2, 1, 3):
            send(ys, yr.at[y], ys_s, yr_s, at(0, dy, 0, 1))
        yr[y] = ys[...]

        drain(down1.at[pl.ds(0, 2)], d1a_rs.at[0])
        b, a = back + 0, ahead + 0
        send(down1.at[b, pl.ds(0, 16)], down1.at[b, pl.ds(0, 16)], d1b_ss, d1b_rs, at(2, 0, 0, 1))
        send(down1.at[a, pl.ds(16, 16)], down1.at[a, pl.ds(16, 16)], d1b_ss, d1b_rs, at(6, 0, 0, 1))
        send(down1.at[b], down1.at[b], d1b_ss, d1b_rs, at(1, 0, 0, 1))
        send(down1.at[a], down1.at[a], d1b_ss, d1b_rs, at(7, 0, 0, 1))

        for dz in (1, 7):
            send(up2y, up2.at[z], u2c_ss, u2c_rs, at(dz, 0, 0, 1))
        drain(yr.at[pl.ds(0, 3)], yr_s)
        preact = jnp.sum(yr[...].astype(F32), axis=0)
        squares = jnp.sum(preact[:, 1024:], axis=1, keepdims=True) / 64
        factor = lax.rsqrt(squares / D + EPS)
        act = jnp.square(jnp.maximum(preact[:, :1024] * factor, 0.0)).astype(BF)

        drain(up2.at[pl.ds(0, 2)], u2a_rs)
        send(up2.at[back, pl.ds(0, 2)], up2.at[back, pl.ds(0, 2)], u2b_ss, u2b_rs, at(2, 0, 0, 1))
        send(up2.at[ahead, pl.ds(2, 2)], up2.at[ahead, pl.ds(2, 2)], u2b_ss, u2b_rs, at(6, 0, 0, 1))
        send(up2.at[back], up2.at[back], u2b_ss, u2b_rs, at(1, 0, 0, 1))
        send(up2.at[ahead], up2.at[ahead], u2b_ss, u2b_rs, at(7, 0, 0, 1))

        drain(down1.at[pl.ds(0, 5)], d1c_rs)
        drain(down1.at[pl.ds(0, 6)], d1b_rs)
        branch = nt(act[:, :512], down1[:8].reshape(256, 512)) + nt(act[:, 512:], down1[8:].reshape(256, 512))
        share = jnp.where(x == 0, RESIDUAL, 0.0)
        xs[...] = (branch + share * u_own).astype(BF)
        for dy in (2, 1, 3, 0):
            for dx in (2, 1, 3, 0):
                if dy or dx:
                    send(xs, xr.at[4 * y + x], xs_s, xr_s, at(0, dy, dx, 1))
        xr[4 * y + x] = xs[...]
        loads[6].wait()
        prepare_down2()
        drain(down2.at[0], give_rs)

        drain(xr.at[pl.ds(0, 15)], xr_s)
        middle = jnp.sum(xr[...].astype(F32).reshape(4, 4, 8, 256), axis=1).astype(BF).astype(F32)
        middle = jnp.concatenate([middle[k] for k in range(4)], axis=1)
        squares = jnp.sum(middle * middle, axis=1, keepdims=True)
        factor = lax.rsqrt(squares / D + EPS)
        middle = middle.astype(BF)
        drain(up2.at[pl.ds(0, 2)], u2c_rs)
        drain(up2.at[pl.ds(0, 3)], u2b_rs)
        pre = []
        for k in range(2):
            rows = jnp.concatenate([up2[a, b, k] for b in range(4) for a in range(8)], axis=0)
            pre.append(nn(middle, rows))
        act = jnp.square(jnp.maximum(jnp.concatenate(pre, axis=1) * factor, 0.0))
        acts[...] = act.astype(BF)

        @pl.when(ra != 0)
        def _():
            send(acts, actr.at[8 * y + z], as_s, ar_s, {"ra": 0, "cb": cb})

        for dz in far + (0,):
            for dy in (2, 1, 3, 0):
                if dz or dy:
                    other = at(dz, dy, 0, 1)

                    @pl.when(other["ra"] != 0)
                    def _():
                        send(acts, actr.at[8 * y + z], as_s, ar_s, other)

        actr[8 * y + z] = acts[...]
        own = jnp.sum(xr[pl.ds(4 * y, 4)].astype(F32), axis=0).astype(BF)
        ms[0] = own[:, :128]
        ms[1] = own[:, 128:]
        for dz in far:
            send(ms.at[lax.div(lax.rem(z + dz, 8), 4)], mr.at[z], ms_s, mr_s, at(dz, 0, 0, 1))
        mr[z] = ms[lax.div(z, 4)]

        drain(actr.at[pl.ds(0, 31)], ar_s)
        weights = jnp.concatenate(
            [down2[k, :, 128 * b : 128 * b + 128] for b in range(4) for k in range(2)], axis=1
        )
        gathered = actr[...].astype(F32).reshape(4, 64, 256)
        gathered = jnp.concatenate([gathered[b] for b in range(4)], axis=1).astype(BF)
        fs[...] = nt(weights, gathered).astype(BF)
        for k in range(4):
            @pl.when(x != k)
            def _():
                send(fs, fr.at[x], fs_s.at[1], fr_s, {"ra": ra, "cb": 2 * k + 1})
        for k in range(4):
            send(fs, fr.at[x], fs_s.at[0], fr_s, {"ra": ra, "cb": 2 * k})
        fr[x] = fs[...]
        drain(mr.at[pl.ds(0, 7)], mr_s)
        mid = mr[...].astype(F32).reshape(64, 128).astype(BF)
        rs[...] = RESIDUAL * nt(place, mid)
        send(rs, rr, rs_s, rr_s, at(0, 0, 0, 0))
        rr[...] = rs[...]
        drain(fr.at[pl.ds(0, 3)], fr_s)
        finish()

        drain(pr1.at[pl.ds(0, 7)], ps_s)
        drain(down1.at[pl.ds(0, 2)], d1a_ss)
        drain(down1.at[pl.ds(0, 2)], d1c_ss)
        drain(down1.at[pl.ds(0, 6)], d1b_ss)
        drain(up2s.at[pl.ds(0, 3)], u1_ss)
        drain(yr.at[pl.ds(0, 3)], ys_s)
        drain(up2.at[pl.ds(0, 2)], u2a_ss)
        drain(up2.at[pl.ds(0, 2)], u2c_ss)
        drain(up2.at[pl.ds(0, 3)], u2b_ss)
        drain(xr.at[pl.ds(0, 15)], xs_s)
        drain(actr.at[pl.ds(0, 31)], as_s)
        drain(mr.at[pl.ds(0, 7)], ms_s)
        drain(rr, rs_s)
        drain(fr, fs_s.at[0])
        drain(fr.at[pl.ds(0, 3)], fs_s.at[1])


def local(stream, gain_first, up_first, down_first, gain_second, up_second, down_second):
    vmem = [
        ((32, 64), BF), ((2, 1, 32), F32), ((2, 32, 512), F32), ((2, 32, 512), F32),
        ((32, 512), BF), ((4, 32, 128), BF), ((2, 32, 512), BF),
        ((8, 8, 640), BF), ((8, 8, 512), BF), ((8, 8, 640), BF), ((8, 1152), BF), ((4, 8, 1152), BF),
        ((16, 32, 512), BF), ((4, 2, 32, 128), BF), ((8, 4, 2, 32, 128), BF),
        ((8, 256), BF), ((16, 8, 256), BF), ((2, 8, 128), BF), ((8, 8, 128), BF),
        ((8, 256), BF), ((32, 8, 256), BF), ((32, 64), BF), ((4, 32, 64), BF),
        ((32, 64), F32), ((32, 64), F32),
    ]
    dma = pltpu.SemaphoreType.DMA
    call = pl.pallas_call(
        kernel,
        out_shape=jax.ShapeDtypeStruct((32, 64), BF),
        in_specs=[pl.BlockSpec(memory_space=pl.ANY)] * 7,
        out_specs=pl.BlockSpec(memory_space=pltpu.VMEM),
        scratch_shapes=[pltpu.VMEM(*v) for v in vmem] + [dma((7,)), dma((2,)), dma((2,))] + [dma(())] * 29
        + [pltpu.SemaphoreType.REGULAR],
        compiler_params=pltpu.CompilerParams(collective_id=0, has_side_effects=True, vmem_limit_bytes=56535040),
    )
    out = call(
        stream.T, gain_first[None], up_first, down_first.T, gain_second[None], up_second, down_second.T
    )
    return out.T


def solution(mesh):
    in_specs = (P(None, "ra"), P("ra"), P("ra", "cb"), P("cb", "ra"), P("ra"), P("ra", "cb"), P("cb", "ra"))
    return jax.shard_map(local, mesh=mesh, in_specs=in_specs, out_specs=P(None, "ra"), check_vma=False)
```

```python
import jax
import jax.numpy as jnp
from jax import lax
from jax.experimental import pallas as pl
from jax.experimental.pallas import tpu as pltpu
from jax.sharding import PartitionSpec as P

D = 1024
EPS = 1e-06
RESIDUAL = 0.25
BF = jnp.bfloat16
F32 = jnp.float32


def nt(a, b):
    return lax.dot_general(a, b, (((1,), (1,)), ((), ())), preferred_element_type=F32)


def nn(a, b):
    return jnp.dot(a, b, preferred_element_type=F32)


def lanes(shape):
    return lax.broadcasted_iota(jnp.int32, shape, len(shape) - 1)


def kernel(
    stream_h, gain_a, up_a, down_a, gain_b, up_b, down_b, out_ref,
    stream_v, gain_v, up_v, down_v,
    down1s, up2s, down2,
    ps, pr0, pr1, ys, yr, down1, up2y, up2, xs, xr, ms, mr, acts, actr, fs, fr, rs, rr,
    load_sem, fs_s, d1a_rs, give_ss, give_rs, ps_s, pr0_s, pr1_s, ys_s, yr_s, d1a_ss, d1b_ss, d1b_rs,
    u1_ss, u1_rs, u2a_ss, u2a_rs, u2b_ss, u2b_rs,
    xs_s, xr_s, ms_s, mr_s, as_s, ar_s, fr_s, rs_s, rr_s, d1c_ss, d1c_rs, u2c_ss, u2c_rs, go,
):
    ra, cb = lax.axis_index("ra"), lax.axis_index("cb")
    z, y = lax.div(ra, 4), lax.rem(ra, 4)
    x, c = lax.div(cb, 2), lax.rem(cb, 2)
    far = (4, 3, 5, 2, 6, 1, 7)
    barrier = pltpu.get_barrier_semaphore()
    loads = [
        pltpu.make_async_copy(src, dst, load_sem.at[k])
        for k, (src, dst) in enumerate(
            [
                (stream_h, stream_v),
                (gain_a, gain_v.at[0]),
                (up_a, up_v.at[0]),
                (down_a, down_v.at[0]),
                (gain_b, gain_v.at[1]),
                (up_b, up_v.at[1]),
                (down_b, down_v.at[1]),
            ]
        )
    ]

    def at(dz, dy, dx, core):
        return {"ra": lax.rem(z + dz, 8) * 4 + lax.rem(y + dy, 4), "cb": lax.rem(x + dx, 4) * 2 + core}

    def send(src, dst, ss, rsem, where):
        pltpu.make_async_remote_copy(
            src_ref=src, dst_ref=dst, send_sem=ss, recv_sem=rsem, device_id=where
        ).start()

    def drain(ref, sem):
        pltpu.make_async_copy(ref, ref, sem).wait()

    def hello(where):
        pl.semaphore_signal(barrier, inc=1, device_id=where)

    def first_up():
        loads[0].wait()
        loads[1].wait()
        u = stream_v[...].astype(F32).T
        loads[2].wait()
        part = nn((u * gain_v[0]).astype(BF), up_v[0].astype(BF))
        ps[:, :, :512] = part.reshape(8, 8, 512).astype(BF)
        return u

    def prepare_up2():
        eye = lax.broadcasted_iota(jnp.int32, (32, 32), 0) == lanes((32, 32))
        loads[4].wait()
        loads[5].wait()
        column = jnp.sum(jnp.where(eye, gain_v[1], 0.0), axis=1, keepdims=True)
        scaled = (up_v[1].astype(BF).astype(F32) * column).astype(BF)
        for k in range(4):
            up2s[k] = scaled[:, 128 * k : 128 * k + 128]

    def prepare_down1():
        loads[3].wait()
        down1s[...] = down_v[0].astype(BF)

    def prepare_down2():
        down2[c] = down_v[1].astype(BF)

    def finish():
        out_ref[...] = (jnp.sum(fr[...].astype(F32), axis=0) + rr[...]).astype(BF)

    @pl.when(c == 0)
    def _():
        for load in loads[:3]:
            load.start()
        for dx in range(4):
            hello(at(0, 0, dx, 1))
        for load in loads[3:]:
            load.start()
        first_up()
        prepare_up2()
        prepare_down1()
        pl.semaphore_wait(barrier, 1)
        pl.semaphore_wait(go, 1)
        for dy in (2, 1, 3, 0):
            send(up2s.at[lax.rem(y + dy, 4)], up2y.at[y, 0], u1_ss, u1_rs, at(0, dy, 0, 1))
        for dz in far + (0,):
            send(ps.at[lax.rem(z + dz, 8), :, pl.ds(0, 512)], pr0.at[z], ps_s, pr0_s, at(dz, 0, 0, 1))
        for dz in (2, 6):
            send(down1s, down1.at[z], d1a_ss, d1a_rs.at[0], at(dz, 0, 0, 1))
        for dz in (1, 7, 0):
            send(down1s, down1.at[z], d1c_ss, d1c_rs, at(dz, 0, 0, 1))
        partner = at(0, 0, 0, 1)
        loads[6].wait()
        prepare_down2()
        send(down2.at[0], down2.at[0], give_ss, give_rs, partner)
        drain(pr0, ps_s)
        drain(down1.at[pl.ds(0, 2)], d1a_ss)
        drain(down1.at[pl.ds(0, 3)], d1c_ss)
        drain(up2s, u1_ss)
        drain(down2.at[0], give_ss)
        drain(rr, rr_s)
        drain(fr, fr_s)
        finish()

    @pl.when(c == 1)
    def _():
        for dz in far:
            hello(at(dz, 0, 0, 1))
        for load in loads[:3]:
            load.start()
        for d in (2, 1, 3):
            hello(at(0, d, 0, 1))
            hello(at(0, 0, d, 1))
        hello(at(0, 0, 0, 0))
        for load in loads[3:]:
            load.start()

        u = first_up()
        place = lanes((32, 128)) == 32 * lax.rem(z, 4) + lax.broadcasted_iota(jnp.int32, (32, 128), 0)
        place = place.astype(F32).astype(BF)
        ps[:, :, 512:] = nn(u.astype(BF), place).reshape(8, 8, 128).astype(BF)
        prepare_up2()
        prepare_down1()

        pl.semaphore_wait(barrier, 17)
        pl.semaphore_signal(go, inc=1, device_id=at(0, 0, 0, 0))
        for dy in (2, 1, 3):
            send(up2s.at[lax.rem(y + dy, 4)], up2y.at[y, 1], u1_ss, u1_rs, at(0, dy, 0, 1))
        for dz in (2, 6):
            send(down1s, down1.at[8 + z], d1a_ss, d1a_rs.at[1], at(dz, 0, 0, 1))
        for dz in far:
            send(ps.at[lax.rem(z + dz, 8)], pr1.at[z], ps_s, pr1_s, at(dz, 0, 0, 1))
        for dz in (1, 7):
            send(down1s, down1.at[8 + z], d1c_ss, d1c_rs, at(dz, 0, 0, 1))
        pr1[z] = ps[z]
        down1[8 + z] = down1s[...]
        up2y[y, 1] = up2s[y]
        drain(down1.at[pl.ds(0, 7), :, pl.ds(0, 128)], u1_rs)
        for dz in (2, 6):
            send(up2y, up2.at[z], u2a_ss, u2a_rs, at(dz, 0, 0, 1))
        up2[z] = up2y[...]
        back, ahead = lax.rem(z + 6, 8), lax.rem(z + 2, 8)
        drain(down1.at[pl.ds(0, 2)], d1a_rs.at[1])
        b, a = back + 8, ahead + 8
        send(down1.at[b, pl.ds(0, 16)], down1.at[b, pl.ds(0, 16)], d1b_ss, d1b_rs, at(2, 0, 0, 1))
        send(down1.at[a, pl.ds(16, 16)], down1.at[a, pl.ds(16, 16)], d1b_ss, d1b_rs, at(6, 0, 0, 1))
        send(down1.at[b], down1.at[b], d1b_ss, d1b_rs, at(1, 0, 0, 1))
        send(down1.at[a], down1.at[a], d1b_ss, d1b_rs, at(7, 0, 0, 1))


        drain(pr0, pr0_s)
        drain(pr1.at[pl.ds(0, 7)], pr1_s)
        partial = [jnp.sum(pr0[...].astype(F32), axis=0), jnp.sum(pr1[:, :, :512].astype(F32), axis=0)]
        u_own = jnp.concatenate(
            [
                jnp.sum(pr1[0:4, :, 512:].astype(F32), axis=0),
                jnp.sum(pr1[4:8, :, 512:].astype(F32), axis=0),
            ],
            axis=1,
        )
        squares = jnp.sum(u_own * u_own, axis=1, keepdims=True)
        high = squares.astype(BF).astype(F32)
        ys[:, :512] = partial[0].astype(BF)
        ys[:, 512:1024] = partial[1].astype(BF)
        ys[:, 1024:] = jnp.where(lanes((8, 128)) < 64, high, squares - high).astype(BF)
        drain(down1.at[pl.ds(0, 2)], d1a_rs.at[0])
        b, a = back + 0, ahead + 0
        send(down1.at[b, pl.ds(0, 16)], down1.at[b, pl.ds(0, 16)], d1b_ss, d1b_rs, at(2, 0, 0, 1))
        send(down1.at[a, pl.ds(16, 16)], down1.at[a, pl.ds(16, 16)], d1b_ss, d1b_rs, at(6, 0, 0, 1))
        send(down1.at[b], down1.at[b], d1b_ss, d1b_rs, at(1, 0, 0, 1))
        send(down1.at[a], down1.at[a], d1b_ss, d1b_rs, at(7, 0, 0, 1))

        for dy in (2, 1, 3):
            send(ys, yr.at[y], ys_s, yr_s, at(0, dy, 0, 1))
        yr[y] = ys[...]

        for dz in (1, 7):
            send(up2y, up2.at[z], u2c_ss, u2c_rs, at(dz, 0, 0, 1))
        drain(yr.at[pl.ds(0, 3)], yr_s)
        preact = jnp.sum(yr[...].astype(F32), axis=0)
        squares = jnp.sum(preact[:, 1024:], axis=1, keepdims=True) / 64
        factor = lax.rsqrt(squares / D + EPS)
        act = jnp.square(jnp.maximum(preact[:, :1024] * factor, 0.0)).astype(BF)

        drain(up2.at[pl.ds(0, 2)], u2a_rs)
        send(up2.at[back, pl.ds(0, 2)], up2.at[back, pl.ds(0, 2)], u2b_ss, u2b_rs, at(2, 0, 0, 1))
        send(up2.at[ahead, pl.ds(2, 2)], up2.at[ahead, pl.ds(2, 2)], u2b_ss, u2b_rs, at(6, 0, 0, 1))
        send(up2.at[back], up2.at[back], u2b_ss, u2b_rs, at(1, 0, 0, 1))
        send(up2.at[ahead], up2.at[ahead], u2b_ss, u2b_rs, at(7, 0, 0, 1))

        drain(down1.at[pl.ds(0, 5)], d1c_rs)
        drain(down1.at[pl.ds(0, 6)], d1b_rs)
        branch = nt(act[:, :512], down1[:8].reshape(256, 512)) + nt(act[:, 512:], down1[8:].reshape(256, 512))
        share = jnp.where(x == 0, RESIDUAL, 0.0)
        xs[...] = (branch + share * u_own).astype(BF)
        for dy in (2, 1, 3, 0):
            for dx in (2, 1, 3, 0):
                if dy or dx:
                    send(xs, xr.at[4 * y + x], xs_s, xr_s, at(0, dy, dx, 1))
        xr[4 * y + x] = xs[...]
        loads[6].wait()
        prepare_down2()
        drain(down2.at[0], give_rs)

        drain(xr.at[pl.ds(0, 15)], xr_s)
        middle = jnp.sum(xr[...].astype(F32).reshape(4, 4, 8, 256), axis=1).astype(BF).astype(F32)
        middle = jnp.concatenate([middle[k] for k in range(4)], axis=1)
        squares = jnp.sum(middle * middle, axis=1, keepdims=True)
        factor = lax.rsqrt(squares / D + EPS)
        middle = middle.astype(BF)
        drain(up2.at[pl.ds(0, 2)], u2c_rs)
        drain(up2.at[pl.ds(0, 3)], u2b_rs)
        pre = []
        for k in range(2):
            rows = jnp.concatenate([up2[a, b, k] for b in range(4) for a in range(8)], axis=0)
            pre.append(nn(middle, rows))
        act = jnp.square(jnp.maximum(jnp.concatenate(pre, axis=1) * factor, 0.0))
        acts[...] = act.astype(BF)

        @pl.when(ra != 0)
        def _():
            send(acts, actr.at[8 * y + z], as_s, ar_s, {"ra": 0, "cb": cb})

        for dz in far + (0,):
            for dy in (2, 1, 3, 0):
                if dz or dy:
                    other = at(dz, dy, 0, 1)

                    @pl.when(other["ra"] != 0)
                    def _():
                        send(acts, actr.at[8 * y + z], as_s, ar_s, other)

        actr[8 * y + z] = acts[...]
        own = jnp.sum(xr[pl.ds(4 * y, 4)].astype(F32), axis=0).astype(BF)
        ms[0] = own[:, :128]
        ms[1] = own[:, 128:]
        for dz in far:
            send(ms.at[lax.div(lax.rem(z + dz, 8), 4)], mr.at[z], ms_s, mr_s, at(dz, 0, 0, 1))
        mr[z] = ms[lax.div(z, 4)]

        weights = jnp.concatenate(
            [down2[k, :, 128 * b : 128 * b + 128] for b in range(4) for k in range(2)], axis=1
        )
        drain(actr.at[pl.ds(0, 31)], ar_s)
        gathered = actr[...].reshape(4, 64, 256)
        gathered = jnp.concatenate([gathered[b] for b in range(4)], axis=1)
        fs[...] = nt(weights, gathered).astype(BF)
        for k in range(4):
            @pl.when(x != k)
            def _():
                send(fs, fr.at[x], fs_s.at[1], fr_s, {"ra": ra, "cb": 2 * k + 1})
        for k in range(4):
            send(fs, fr.at[x], fs_s.at[0], fr_s, {"ra": ra, "cb": 2 * k})
        fr[x] = fs[...]
        drain(mr.at[pl.ds(0, 7)], mr_s)
        mid = mr[...].astype(F32).reshape(64, 128).astype(BF)
        rs[...] = RESIDUAL * nt(place, mid)
        send(rs, rr, rs_s, rr_s, at(0, 0, 0, 0))
        rr[...] = rs[...]
        drain(fr.at[pl.ds(0, 3)], fr_s)
        finish()

        drain(pr1.at[pl.ds(0, 7)], ps_s)
        drain(down1.at[pl.ds(0, 2)], d1a_ss)
        drain(down1.at[pl.ds(0, 2)], d1c_ss)
        drain(down1.at[pl.ds(0, 6)], d1b_ss)
        drain(up2s.at[pl.ds(0, 3)], u1_ss)
        drain(yr.at[pl.ds(0, 3)], ys_s)
        drain(up2.at[pl.ds(0, 2)], u2a_ss)
        drain(up2.at[pl.ds(0, 2)], u2c_ss)
        drain(up2.at[pl.ds(0, 3)], u2b_ss)
        drain(xr.at[pl.ds(0, 15)], xs_s)
        drain(actr.at[pl.ds(0, 31)], as_s)
        drain(mr.at[pl.ds(0, 7)], ms_s)
        drain(rr, rs_s)
        drain(fr, fs_s.at[0])
        drain(fr.at[pl.ds(0, 3)], fs_s.at[1])


def local(stream, gain_first, up_first, down_first, gain_second, up_second, down_second):
    vmem = [
        ((32, 64), BF), ((2, 1, 32), F32), ((2, 32, 512), F32), ((2, 32, 512), F32),
        ((32, 512), BF), ((4, 32, 128), BF), ((2, 32, 512), BF),
        ((8, 8, 640), BF), ((8, 8, 512), BF), ((8, 8, 640), BF), ((8, 1152), BF), ((4, 8, 1152), BF),
        ((16, 32, 512), BF), ((4, 2, 32, 128), BF), ((8, 4, 2, 32, 128), BF),
        ((8, 256), BF), ((16, 8, 256), BF), ((2, 8, 128), BF), ((8, 8, 128), BF),
        ((8, 256), BF), ((32, 8, 256), BF), ((32, 64), BF), ((4, 32, 64), BF),
        ((32, 64), F32), ((32, 64), F32),
    ]
    dma = pltpu.SemaphoreType.DMA
    call = pl.pallas_call(
        kernel,
        out_shape=jax.ShapeDtypeStruct((32, 64), BF),
        in_specs=[pl.BlockSpec(memory_space=pl.ANY)] * 7,
        out_specs=pl.BlockSpec(memory_space=pltpu.VMEM),
        scratch_shapes=[pltpu.VMEM(*v) for v in vmem] + [dma((7,)), dma((2,)), dma((2,))] + [dma(())] * 29
        + [pltpu.SemaphoreType.REGULAR],
        compiler_params=pltpu.CompilerParams(collective_id=0, has_side_effects=True, vmem_limit_bytes=56535040),
    )
    out = call(
        stream.T, gain_first[None], up_first, down_first.T, gain_second[None], up_second, down_second.T
    )
    return out.T


def solution(mesh):
    in_specs = (P(None, "ra"), P("ra"), P("ra", "cb"), P("cb", "ra"), P("ra"), P("ra", "cb"), P("cb", "ra"))
    return jax.shard_map(local, mesh=mesh, in_specs=in_specs, out_specs=P(None, "ra"), check_vma=False)
```

```python
import jax
import jax.numpy as jnp
from jax import lax
from jax.experimental import pallas as pl
from jax.experimental.pallas import tpu as pltpu
from jax.sharding import PartitionSpec as P

D = 1024
EPS = 1e-06
RESIDUAL = 0.25
BF = jnp.bfloat16
F32 = jnp.float32


def nt(a, b):
    return lax.dot_general(a, b, (((1,), (1,)), ((), ())), preferred_element_type=F32)


def nn(a, b):
    return jnp.dot(a, b, preferred_element_type=F32)


def lanes(shape):
    return lax.broadcasted_iota(jnp.int32, shape, len(shape) - 1)


def kernel(
    stream_h, gain_a, up_a, down_a, gain_b, up_b, down_b, out_ref,
    stream_v, gain_v, up_v, down_v,
    down1s, up2s, down2,
    ps, pr0, pr1, ys, yr, down1, up2y, up2, xs, xr, ms, mr, acts, actr, fs, fr, rs, rr,
    load_sem, fs_s, d1a_rs, give_ss, give_rs, ps_s, pr0_s, pr1_s, ys_s, yr_s, d1a_ss, d1b_ss, d1b_rs,
    u1_ss, u1_rs, u2a_ss, u2a_rs, u2b_ss, u2b_rs,
    xs_s, xr_s, ms_s, mr_s, as_s, ar_s, fr_s, rs_s, rr_s, d1c_ss, d1c_rs, u2c_ss, u2c_rs, go,
):
    ra, cb = lax.axis_index("ra"), lax.axis_index("cb")
    z, y = lax.div(ra, 4), lax.rem(ra, 4)
    x, c = lax.div(cb, 2), lax.rem(cb, 2)
    far = (4, 3, 5, 2, 6, 1, 7)
    barrier = pltpu.get_barrier_semaphore()
    loads = [
        pltpu.make_async_copy(src, dst, load_sem.at[k])
        for k, (src, dst) in enumerate(
            [
                (stream_h, stream_v),
                (gain_a, gain_v.at[0]),
                (up_a, up_v.at[0]),
                (down_a, down_v.at[0]),
                (gain_b, gain_v.at[1]),
                (up_b, up_v.at[1]),
                (down_b, down_v.at[1]),
            ]
        )
    ]

    def at(dz, dy, dx, core):
        return {"ra": lax.rem(z + dz, 8) * 4 + lax.rem(y + dy, 4), "cb": lax.rem(x + dx, 4) * 2 + core}

    def send(src, dst, ss, rsem, where):
        pltpu.make_async_remote_copy(
            src_ref=src, dst_ref=dst, send_sem=ss, recv_sem=rsem, device_id=where
        ).start()

    def drain(ref, sem):
        pltpu.make_async_copy(ref, ref, sem).wait()

    def hello(where):
        pl.semaphore_signal(barrier, inc=1, device_id=where)

    def first_up():
        loads[0].wait()
        loads[1].wait()
        u = stream_v[...].astype(F32).T
        loads[2].wait()
        part = nn((u * gain_v[0]).astype(BF), up_v[0].astype(BF))
        ps[:, :, :512] = part.reshape(8, 8, 512).astype(BF)
        return u

    def prepare_up2():
        eye = lax.broadcasted_iota(jnp.int32, (32, 32), 0) == lanes((32, 32))
        loads[4].wait()
        loads[5].wait()
        column = jnp.sum(jnp.where(eye, gain_v[1], 0.0), axis=1, keepdims=True)
        scaled = (up_v[1].astype(BF).astype(F32) * column).astype(BF)
        for k in range(4):
            up2s[k] = scaled[:, 128 * k : 128 * k + 128]

    def prepare_down1():
        loads[3].wait()
        down1s[...] = down_v[0].astype(BF)

    def prepare_down2():
        down2[c] = down_v[1].astype(BF)

    def finish():
        out_ref[...] = (jnp.sum(fr[...].astype(F32), axis=0) + rr[...]).astype(BF)

    @pl.when(c == 0)
    def _():
        for load in loads[:3]:
            load.start()
        for dx in range(4):
            hello(at(0, 0, dx, 1))
        for load in loads[3:]:
            load.start()
        first_up()
        prepare_up2()
        prepare_down1()
        pl.semaphore_wait(barrier, 1)
        pl.semaphore_wait(go, 1)
        for dy in (2, 1, 3, 0):
            send(up2s.at[lax.rem(y + dy, 4)], up2y.at[y, 0], u1_ss, u1_rs, at(0, dy, 0, 1))
        for dz in far + (0,):
            send(ps.at[lax.rem(z + dz, 8), :, pl.ds(0, 512)], pr0.at[z], ps_s, pr0_s, at(dz, 0, 0, 1))
        for dz in (2, 6):
            send(down1s, down1.at[z], d1a_ss, d1a_rs.at[0], at(dz, 0, 0, 1))
        for dz in (1, 7, 0):
            send(down1s, down1.at[z], d1c_ss, d1c_rs, at(dz, 0, 0, 1))
        partner = at(0, 0, 0, 1)
        loads[6].wait()
        prepare_down2()
        send(down2.at[0], down2.at[0], give_ss, give_rs, partner)
        drain(pr0, ps_s)
        drain(down1.at[pl.ds(0, 2)], d1a_ss)
        drain(down1.at[pl.ds(0, 3)], d1c_ss)
        drain(up2s, u1_ss)
        drain(down2.at[0], give_ss)
        drain(rr, rr_s)
        drain(fr, fr_s)
        finish()

    @pl.when(c == 1)
    def _():
        for dz in far:
            hello(at(dz, 0, 0, 1))
        for load in loads[:3]:
            load.start()
        for d in (2, 1, 3):
            hello(at(0, d, 0, 1))
            hello(at(0, 0, d, 1))
        hello(at(0, 0, 0, 0))
        for load in loads[3:]:
            load.start()

        u = first_up()
        place = lanes((32, 128)) == 32 * lax.rem(z, 4) + lax.broadcasted_iota(jnp.int32, (32, 128), 0)
        place = place.astype(F32).astype(BF)
        ps[:, :, 512:] = nn(u.astype(BF), place).reshape(8, 8, 128).astype(BF)
        prepare_up2()
        prepare_down1()

        pl.semaphore_wait(barrier, 17)
        pl.semaphore_signal(go, inc=1, device_id=at(0, 0, 0, 0))
        for dy in (2, 1, 3):
            send(up2s.at[lax.rem(y + dy, 4)], up2y.at[y, 1], u1_ss, u1_rs, at(0, dy, 0, 1))
        for dz in (2, 6):
            send(down1s, down1.at[8 + z], d1a_ss, d1a_rs.at[1], at(dz, 0, 0, 1))
        for dz in far:
            send(ps.at[lax.rem(z + dz, 8)], pr1.at[z], ps_s, pr1_s, at(dz, 0, 0, 1))
        for dz in (1, 7):
            send(down1s, down1.at[8 + z], d1c_ss, d1c_rs, at(dz, 0, 0, 1))
        pr1[z] = ps[z]
        down1[8 + z] = down1s[...]
        up2y[y, 1] = up2s[y]
        drain(down1.at[pl.ds(0, 7), :, pl.ds(0, 128)], u1_rs)
        for dz in (2, 6):
            send(up2y, up2.at[z], u2a_ss, u2a_rs, at(dz, 0, 0, 1))
        up2[z] = up2y[...]
        back, ahead = lax.rem(z + 6, 8), lax.rem(z + 2, 8)
        drain(down1.at[pl.ds(0, 2)], d1a_rs.at[1])
        b, a = back + 8, ahead + 8
        send(down1.at[b, pl.ds(0, 16)], down1.at[b, pl.ds(0, 16)], d1b_ss, d1b_rs, at(2, 0, 0, 1))
        send(down1.at[a, pl.ds(16, 16)], down1.at[a, pl.ds(16, 16)], d1b_ss, d1b_rs, at(6, 0, 0, 1))
        send(down1.at[b], down1.at[b], d1b_ss, d1b_rs, at(1, 0, 0, 1))
        send(down1.at[a], down1.at[a], d1b_ss, d1b_rs, at(7, 0, 0, 1))


        drain(pr0, pr0_s)
        drain(pr1.at[pl.ds(0, 7)], pr1_s)
        partial = [jnp.sum(pr0[...].astype(F32), axis=0), jnp.sum(pr1[:, :, :512].astype(F32), axis=0)]
        u_own = jnp.concatenate(
            [
                jnp.sum(pr1[0:4, :, 512:].astype(F32), axis=0),
                jnp.sum(pr1[4:8, :, 512:].astype(F32), axis=0),
            ],
            axis=1,
        )
        squares = jnp.sum(u_own * u_own, axis=1, keepdims=True)
        high = squares.astype(BF).astype(F32)
        ys[:, :512] = partial[0].astype(BF)
        ys[:, 512:1024] = partial[1].astype(BF)
        ys[:, 1024:] = jnp.where(lanes((8, 128)) < 64, high, squares - high).astype(BF)
        drain(down1.at[pl.ds(0, 2)], d1a_rs.at[0])
        b, a = back + 0, ahead + 0
        send(down1.at[b, pl.ds(0, 16)], down1.at[b, pl.ds(0, 16)], d1b_ss, d1b_rs, at(2, 0, 0, 1))
        send(down1.at[a, pl.ds(16, 16)], down1.at[a, pl.ds(16, 16)], d1b_ss, d1b_rs, at(6, 0, 0, 1))
        send(down1.at[b], down1.at[b], d1b_ss, d1b_rs, at(1, 0, 0, 1))
        send(down1.at[a], down1.at[a], d1b_ss, d1b_rs, at(7, 0, 0, 1))

        for dy in (2, 1, 3):
            send(ys, yr.at[y], ys_s, yr_s, at(0, dy, 0, 1))
        yr[y] = ys[...]

        for dz in (1, 7):
            send(up2y, up2.at[z], u2c_ss, u2c_rs, at(dz, 0, 0, 1))
        drain(yr.at[pl.ds(0, 3)], yr_s)
        preact = jnp.sum(yr[...].astype(F32), axis=0)
        squares = jnp.sum(preact[:, 1024:], axis=1, keepdims=True) / 64
        factor = lax.rsqrt(squares / D + EPS)
        act = jnp.square(jnp.maximum(preact[:, :1024] * factor, 0.0)).astype(BF)

        drain(up2.at[pl.ds(0, 2)], u2a_rs)
        send(up2.at[back, pl.ds(0, 2)], up2.at[back, pl.ds(0, 2)], u2b_ss, u2b_rs, at(2, 0, 0, 1))
        send(up2.at[ahead, pl.ds(2, 2)], up2.at[ahead, pl.ds(2, 2)], u2b_ss, u2b_rs, at(6, 0, 0, 1))
        send(up2.at[back], up2.at[back], u2b_ss, u2b_rs, at(1, 0, 0, 1))
        send(up2.at[ahead], up2.at[ahead], u2b_ss, u2b_rs, at(7, 0, 0, 1))

        drain(down1.at[pl.ds(0, 5)], d1c_rs)
        drain(down1.at[pl.ds(0, 6)], d1b_rs)
        branch = nt(act[:, :512], down1[:8].reshape(256, 512)) + nt(act[:, 512:], down1[8:].reshape(256, 512))
        share = jnp.where(x == 0, RESIDUAL, 0.0)
        xs[...] = (branch + share * u_own).astype(BF)
        for dy in (2, 1, 3, 0):
            for dx in (2, 1, 3, 0):
                if dy or dx:
                    send(xs, xr.at[4 * y + x], xs_s, xr_s, at(0, dy, dx, 1))
        xr[4 * y + x] = xs[...]
        loads[6].wait()
        prepare_down2()
        drain(down2.at[0], give_rs)

        drain(xr.at[pl.ds(0, 15)], xr_s)
        middle = jnp.sum(xr[...].astype(F32).reshape(4, 4, 8, 256), axis=1).astype(BF).astype(F32)
        middle = jnp.concatenate([middle[k] for k in range(4)], axis=1)
        squares = jnp.sum(middle * middle, axis=1, keepdims=True)
        factor = lax.rsqrt(squares / D + EPS)
        middle = middle.astype(BF)
        drain(up2.at[pl.ds(0, 2)], u2c_rs)
        drain(up2.at[pl.ds(0, 3)], u2b_rs)
        pre = []
        for k in range(2):
            rows = jnp.concatenate([up2[a, b, k] for b in range(4) for a in range(8)], axis=0)
            pre.append(nn(middle, rows))
        act = jnp.square(jnp.maximum(jnp.concatenate(pre, axis=1) * factor, 0.0))
        acts[...] = act.astype(BF)

        @pl.when(ra != 0)
        def _():
            send(acts, actr.at[8 * y + z], as_s, ar_s, {"ra": 0, "cb": cb})

        for dz in far + (0,):
            for dy in (2, 1, 3, 0):
                if dz or dy:
                    other = at(dz, dy, 0, 1)

                    @pl.when(other["ra"] != 0)
                    def _():
                        send(acts, actr.at[8 * y + z], as_s, ar_s, other)

        actr[8 * y + z] = acts[...]
        own = jnp.sum(xr[pl.ds(4 * y, 4)].astype(F32), axis=0).astype(BF)
        ms[0] = own[:, :128]
        ms[1] = own[:, 128:]
        for dz in far:
            send(ms.at[lax.div(lax.rem(z + dz, 8), 4)], mr.at[z], ms_s, mr_s, at(dz, 0, 0, 1))
        mr[z] = ms[lax.div(z, 4)]

        weights = jnp.concatenate(
            [down2[k, :, 128 * b : 128 * b + 128] for b in range(4) for k in range(2)], axis=1
        )
        drain(actr.at[pl.ds(0, 31)], ar_s)
        gathered = actr[...].reshape(4, 64, 256)
        gathered = jnp.concatenate([gathered[b] for b in range(4)], axis=1)
        fs[...] = nt(weights, gathered).astype(BF)
        for k in range(4):
            @pl.when(x != k)
            def _():
                send(fs, fr.at[x], fs_s.at[1], fr_s, {"ra": ra, "cb": 2 * k + 1})
        for k in range(4):
            send(fs, fr.at[x], fs_s.at[0], fr_s, {"ra": ra, "cb": 2 * k})
        fr[x] = fs[...]
        drain(mr.at[pl.ds(0, 7)], mr_s)
        mid = mr[...].astype(F32).reshape(64, 128).astype(BF)
        rs[...] = RESIDUAL * nt(place, mid)
        send(rs, rr, rs_s, rr_s, at(0, 0, 0, 0))
        rr[...] = rs[...]
        drain(fr.at[pl.ds(0, 3)], fr_s)
        finish()

        drain(pr1.at[pl.ds(0, 7)], ps_s)
        drain(down1.at[pl.ds(0, 2)], d1a_ss)
        drain(down1.at[pl.ds(0, 2)], d1c_ss)
        drain(down1.at[pl.ds(0, 6)], d1b_ss)
        drain(up2s.at[pl.ds(0, 3)], u1_ss)
        drain(yr.at[pl.ds(0, 3)], ys_s)
        drain(up2.at[pl.ds(0, 2)], u2a_ss)
        drain(up2.at[pl.ds(0, 2)], u2c_ss)
        drain(up2.at[pl.ds(0, 3)], u2b_ss)
        drain(xr.at[pl.ds(0, 15)], xs_s)
        drain(actr.at[pl.ds(0, 31)], as_s)
        drain(mr.at[pl.ds(0, 7)], ms_s)
        drain(rr, rs_s)
        drain(fr, fs_s.at[0])
        drain(fr.at[pl.ds(0, 3)], fs_s.at[1])


def local(stream, gain_first, up_first, down_first, gain_second, up_second, down_second):
    vmem = [
        ((32, 64), BF), ((2, 1, 32), F32), ((2, 32, 512), F32), ((2, 32, 512), F32),
        ((32, 512), BF), ((4, 32, 128), BF), ((2, 32, 512), BF),
        ((8, 8, 640), BF), ((8, 8, 512), BF), ((8, 8, 640), BF), ((8, 1152), BF), ((4, 8, 1152), BF),
        ((16, 32, 512), BF), ((4, 2, 32, 128), BF), ((8, 4, 2, 32, 128), BF),
        ((8, 256), BF), ((16, 8, 256), BF), ((2, 8, 128), BF), ((8, 8, 128), BF),
        ((8, 256), BF), ((32, 8, 256), BF), ((32, 64), BF), ((4, 32, 64), BF),
        ((32, 64), F32), ((32, 64), F32),
    ]
    dma = pltpu.SemaphoreType.DMA
    call = pl.pallas_call(
        kernel,
        out_shape=jax.ShapeDtypeStruct((32, 64), BF),
        in_specs=[pl.BlockSpec(memory_space=pl.ANY)] * 7,
        out_specs=pl.BlockSpec(memory_space=pltpu.VMEM),
        scratch_shapes=[pltpu.VMEM(*v) for v in vmem] + [dma((7,)), dma((2,)), dma((2,))] + [dma(())] * 29
        + [pltpu.SemaphoreType.REGULAR],
        compiler_params=pltpu.CompilerParams(collective_id=0, has_side_effects=True, vmem_limit_bytes=56528896),
    )
    out = call(
        stream.T, gain_first[None], up_first, down_first.T, gain_second[None], up_second, down_second.T
    )
    return out.T


def solution(mesh):
    in_specs = (P(None, "ra"), P("ra"), P("ra", "cb"), P("cb", "ra"), P("ra"), P("ra", "cb"), P("cb", "ra"))
    return jax.shard_map(local, mesh=mesh, in_specs=in_specs, out_specs=P(None, "ra"), check_vma=False)
```

```python
import jax
import jax.numpy as jnp
from jax import lax
from jax.experimental import pallas as pl
from jax.experimental.pallas import tpu as pltpu
from jax.sharding import PartitionSpec as P

D = 1024
EPS = 1e-06
RESIDUAL = 0.25
BF = jnp.bfloat16
F32 = jnp.float32


def nt(a, b):
    return lax.dot_general(a, b, (((1,), (1,)), ((), ())), preferred_element_type=F32)


def nn(a, b):
    return jnp.dot(a, b, preferred_element_type=F32)


def lanes(shape):
    return lax.broadcasted_iota(jnp.int32, shape, len(shape) - 1)


def kernel(
    stream_h, gain_a, up_a, down_a, gain_b, up_b, down_b, out_ref,
    stream_v, gain_v, up_v, down_v,
    down1s, up2s, down2,
    ps, pr0, pr1, ys, yr, down1, up2y, up2, xs, xr, ms, mr, acts, actr, fs, fr, rs, rr,
    load_sem, fs_s, d1a_rs, give_ss, give_rs, ps_s, pr0_s, pr1_s, ys_s, yr_s, d1a_ss, d1b_ss, d1b_rs,
    u1_ss, u1_rs, u2a_ss, u2a_rs, u2b_ss, u2b_rs,
    xs_s, xr_s, ms_s, mr_s, as_s, ar_s, fr_s, rs_s, rr_s, d1c_ss, d1c_rs, u2c_ss, u2c_rs, go,
):
    ra, cb = lax.axis_index("ra"), lax.axis_index("cb")
    z, y = lax.div(ra, 4), lax.rem(ra, 4)
    x, c = lax.div(cb, 2), lax.rem(cb, 2)
    far = (4, 3, 5, 2, 6, 1, 7)
    barrier = pltpu.get_barrier_semaphore()
    loads = [
        pltpu.make_async_copy(src, dst, load_sem.at[k])
        for k, (src, dst) in enumerate(
            [
                (stream_h, stream_v),
                (gain_a, gain_v.at[0]),
                (up_a, up_v.at[0]),
                (down_a, down_v.at[0]),
                (gain_b, gain_v.at[1]),
                (up_b, up_v.at[1]),
                (down_b, down_v.at[1]),
            ]
        )
    ]

    def at(dz, dy, dx, core):
        return {"ra": lax.rem(z + dz, 8) * 4 + lax.rem(y + dy, 4), "cb": lax.rem(x + dx, 4) * 2 + core}

    def send(src, dst, ss, rsem, where):
        pltpu.make_async_remote_copy(
            src_ref=src, dst_ref=dst, send_sem=ss, recv_sem=rsem, device_id=where
        ).start()

    def drain(ref, sem):
        pltpu.make_async_copy(ref, ref, sem).wait()

    def hello(where):
        pl.semaphore_signal(barrier, inc=1, device_id=where)

    def first_up():
        loads[0].wait()
        loads[1].wait()
        u = stream_v[...].astype(F32).T
        loads[2].wait()
        part = nn((u * gain_v[0]).astype(BF), up_v[0].astype(BF))
        ps[:, :, :512] = part.reshape(8, 8, 512).astype(BF)
        return u

    def prepare_up2():
        eye = lax.broadcasted_iota(jnp.int32, (32, 32), 0) == lanes((32, 32))
        loads[4].wait()
        loads[5].wait()
        column = jnp.sum(jnp.where(eye, gain_v[1], 0.0), axis=1, keepdims=True)
        scaled = (up_v[1].astype(BF).astype(F32) * column).astype(BF)
        for k in range(4):
            up2s[k] = scaled[:, 128 * k : 128 * k + 128]

    def prepare_down1():
        loads[3].wait()
        down1s[...] = down_v[0].astype(BF)

    def prepare_down2():
        down2[c] = down_v[1].astype(BF)

    def finish():
        out_ref[...] = (jnp.sum(fr[...].astype(F32), axis=0) + rr[...]).astype(BF)

    @pl.when(c == 0)
    def _():
        for load in loads[:3]:
            load.start()
        for dx in range(4):
            hello(at(0, 0, dx, 1))
        for load in loads[3:]:
            load.start()
        first_up()
        prepare_up2()
        prepare_down1()
        pl.semaphore_wait(barrier, 1)
        pl.semaphore_wait(go, 1)
        for dy in (2, 1, 3, 0):
            send(up2s.at[lax.rem(y + dy, 4)], up2y.at[y, 0], u1_ss, u1_rs, at(0, dy, 0, 1))
        for dz in far + (0,):
            send(ps.at[lax.rem(z + dz, 8), :, pl.ds(0, 512)], pr0.at[z], ps_s, pr0_s, at(dz, 0, 0, 1))
        for dz in (2, 6):
            send(down1s, down1.at[z], d1a_ss, d1a_rs.at[0], at(dz, 0, 0, 1))
        for dz in (1, 7, 0):
            send(down1s, down1.at[z], d1c_ss, d1c_rs, at(dz, 0, 0, 1))
        partner = at(0, 0, 0, 1)
        loads[6].wait()
        prepare_down2()
        send(down2.at[0], down2.at[0], give_ss, give_rs, partner)
        drain(pr0, ps_s)
        drain(down1.at[pl.ds(0, 2)], d1a_ss)
        drain(down1.at[pl.ds(0, 3)], d1c_ss)
        drain(up2s, u1_ss)
        drain(down2.at[0], give_ss)
        drain(rr, rr_s)
        drain(fr, fr_s)
        finish()

    @pl.when(c == 1)
    def _():
        for dz in far:
            hello(at(dz, 0, 0, 1))
        for load in loads[:3]:
            load.start()
        for d in (2, 1, 3):
            hello(at(0, d, 0, 1))
            hello(at(0, 0, d, 1))
        hello(at(0, 0, 0, 0))
        for load in loads[3:]:
            load.start()

        u = first_up()
        place = lanes((32, 128)) == 32 * lax.rem(z, 4) + lax.broadcasted_iota(jnp.int32, (32, 128), 0)
        place = place.astype(F32).astype(BF)
        ps[:, :, 512:] = nn(u.astype(BF), place).reshape(8, 8, 128).astype(BF)
        prepare_up2()
        prepare_down1()

        pl.semaphore_wait(barrier, 17)
        pl.semaphore_signal(go, inc=1, device_id=at(0, 0, 0, 0))
        for dy in (2, 1, 3):
            send(up2s.at[lax.rem(y + dy, 4)], up2y.at[y, 1], u1_ss, u1_rs, at(0, dy, 0, 1))
        for dz in (2, 6):
            send(down1s, down1.at[8 + z], d1a_ss, d1a_rs.at[1], at(dz, 0, 0, 1))
        for dz in (4, 5, 3, 6, 2, 7, 1):
            send(ps.at[lax.rem(z + dz, 8)], pr1.at[z], ps_s, pr1_s, at(dz, 0, 0, 1))
        for dz in (1, 7):
            send(down1s, down1.at[8 + z], d1c_ss, d1c_rs, at(dz, 0, 0, 1))
        pr1[z] = ps[z]
        down1[8 + z] = down1s[...]
        up2y[y, 1] = up2s[y]
        drain(down1.at[pl.ds(0, 7), :, pl.ds(0, 128)], u1_rs)
        for dz in (2, 6):
            send(up2y, up2.at[z], u2a_ss, u2a_rs, at(dz, 0, 0, 1))
        up2[z] = up2y[...]
        back, ahead = lax.rem(z + 6, 8), lax.rem(z + 2, 8)
        drain(down1.at[pl.ds(0, 2)], d1a_rs.at[1])
        b, a = back + 8, ahead + 8
        send(down1.at[b, pl.ds(0, 16)], down1.at[b, pl.ds(0, 16)], d1b_ss, d1b_rs, at(2, 0, 0, 1))
        send(down1.at[a, pl.ds(16, 16)], down1.at[a, pl.ds(16, 16)], d1b_ss, d1b_rs, at(6, 0, 0, 1))
        send(down1.at[b], down1.at[b], d1b_ss, d1b_rs, at(1, 0, 0, 1))
        send(down1.at[a], down1.at[a], d1b_ss, d1b_rs, at(7, 0, 0, 1))


        drain(pr0, pr0_s)
        drain(pr1.at[pl.ds(0, 7)], pr1_s)
        partial = [jnp.sum(pr0[...].astype(F32), axis=0), jnp.sum(pr1[:, :, :512].astype(F32), axis=0)]
        u_own = jnp.concatenate(
            [
                jnp.sum(pr1[0:4, :, 512:].astype(F32), axis=0),
                jnp.sum(pr1[4:8, :, 512:].astype(F32), axis=0),
            ],
            axis=1,
        )
        squares = jnp.sum(u_own * u_own, axis=1, keepdims=True)
        high = squares.astype(BF).astype(F32)
        ys[:, :512] = partial[0].astype(BF)
        ys[:, 512:1024] = partial[1].astype(BF)
        ys[:, 1024:] = jnp.where(lanes((8, 128)) < 64, high, squares - high).astype(BF)
        drain(down1.at[pl.ds(0, 2)], d1a_rs.at[0])
        b, a = back + 0, ahead + 0
        send(down1.at[b, pl.ds(0, 16)], down1.at[b, pl.ds(0, 16)], d1b_ss, d1b_rs, at(2, 0, 0, 1))
        send(down1.at[a, pl.ds(16, 16)], down1.at[a, pl.ds(16, 16)], d1b_ss, d1b_rs, at(6, 0, 0, 1))
        send(down1.at[b], down1.at[b], d1b_ss, d1b_rs, at(1, 0, 0, 1))
        send(down1.at[a], down1.at[a], d1b_ss, d1b_rs, at(7, 0, 0, 1))

        for dy in (2, 1, 3):
            send(ys, yr.at[y], ys_s, yr_s, at(0, dy, 0, 1))
        yr[y] = ys[...]

        for dz in (1, 7):
            send(up2y, up2.at[z], u2c_ss, u2c_rs, at(dz, 0, 0, 1))
        drain(yr.at[pl.ds(0, 3)], yr_s)
        preact = jnp.sum(yr[...].astype(F32), axis=0)
        squares = jnp.sum(preact[:, 1024:], axis=1, keepdims=True) / 64
        factor = lax.rsqrt(squares / D + EPS)
        act = jnp.square(jnp.maximum(preact[:, :1024] * factor, 0.0)).astype(BF)

        drain(up2.at[pl.ds(0, 2)], u2a_rs)
        send(up2.at[back, pl.ds(0, 2)], up2.at[back, pl.ds(0, 2)], u2b_ss, u2b_rs, at(2, 0, 0, 1))
        send(up2.at[ahead, pl.ds(2, 2)], up2.at[ahead, pl.ds(2, 2)], u2b_ss, u2b_rs, at(6, 0, 0, 1))
        send(up2.at[back], up2.at[back], u2b_ss, u2b_rs, at(1, 0, 0, 1))
        send(up2.at[ahead], up2.at[ahead], u2b_ss, u2b_rs, at(7, 0, 0, 1))

        drain(down1.at[pl.ds(0, 5)], d1c_rs)
        drain(down1.at[pl.ds(0, 6)], d1b_rs)
        branch = nt(act[:, :512], down1[:8].reshape(256, 512)) + nt(act[:, 512:], down1[8:].reshape(256, 512))
        share = jnp.where(x == 0, RESIDUAL, 0.0)
        xs[...] = (branch + share * u_own).astype(BF)
        for dy in (2, 1, 3, 0):
            for dx in (2, 1, 3, 0):
                if dy or dx:
                    send(xs, xr.at[4 * y + x], xs_s, xr_s, at(0, dy, dx, 1))
        xr[4 * y + x] = xs[...]
        loads[6].wait()
        prepare_down2()
        drain(down2.at[0], give_rs)

        drain(xr.at[pl.ds(0, 15)], xr_s)
        middle = jnp.sum(xr[...].astype(F32).reshape(4, 4, 8, 256), axis=1).astype(BF).astype(F32)
        middle = jnp.concatenate([middle[k] for k in range(4)], axis=1)
        squares = jnp.sum(middle * middle, axis=1, keepdims=True)
        factor = lax.rsqrt(squares / D + EPS)
        middle = middle.astype(BF)
        drain(up2.at[pl.ds(0, 2)], u2c_rs)
        drain(up2.at[pl.ds(0, 3)], u2b_rs)
        pre = []
        for k in range(2):
            rows = jnp.concatenate([up2[a, b, k] for b in range(4) for a in range(8)], axis=0)
            pre.append(nn(middle, rows))
        act = jnp.square(jnp.maximum(jnp.concatenate(pre, axis=1) * factor, 0.0))
        acts[...] = act.astype(BF)

        @pl.when(ra != 0)
        def _():
            send(acts, actr.at[8 * y + z], as_s, ar_s, {"ra": 0, "cb": cb})

        for dz in far + (0,):
            for dy in (2, 1, 3, 0):
                if dz or dy:
                    other = at(dz, dy, 0, 1)

                    @pl.when(other["ra"] != 0)
                    def _():
                        send(acts, actr.at[8 * y + z], as_s, ar_s, other)

        actr[8 * y + z] = acts[...]
        own = jnp.sum(xr[pl.ds(4 * y, 4)].astype(F32), axis=0).astype(BF)
        ms[0] = own[:, :128]
        ms[1] = own[:, 128:]
        for dz in far:
            send(ms.at[lax.div(lax.rem(z + dz, 8), 4)], mr.at[z], ms_s, mr_s, at(dz, 0, 0, 1))
        mr[z] = ms[lax.div(z, 4)]

        weights = jnp.concatenate(
            [down2[k, :, 128 * b : 128 * b + 128] for b in range(4) for k in range(2)], axis=1
        )
        drain(actr.at[pl.ds(0, 31)], ar_s)
        gathered = actr[...].reshape(4, 64, 256)
        gathered = jnp.concatenate([gathered[b] for b in range(4)], axis=1)
        fs[...] = nt(weights, gathered).astype(BF)
        for k in range(4):
            @pl.when(x != k)
            def _():
                send(fs, fr.at[x], fs_s.at[1], fr_s, {"ra": ra, "cb": 2 * k + 1})
        for k in range(4):
            send(fs, fr.at[x], fs_s.at[0], fr_s, {"ra": ra, "cb": 2 * k})
        fr[x] = fs[...]
        drain(mr.at[pl.ds(0, 7)], mr_s)
        mid = mr[...].astype(F32).reshape(64, 128).astype(BF)
        rs[...] = RESIDUAL * nt(place, mid)
        send(rs, rr, rs_s, rr_s, at(0, 0, 0, 0))
        rr[...] = rs[...]
        drain(fr.at[pl.ds(0, 3)], fr_s)
        finish()

        drain(pr1.at[pl.ds(0, 7)], ps_s)
        drain(down1.at[pl.ds(0, 2)], d1a_ss)
        drain(down1.at[pl.ds(0, 2)], d1c_ss)
        drain(down1.at[pl.ds(0, 6)], d1b_ss)
        drain(up2s.at[pl.ds(0, 3)], u1_ss)
        drain(yr.at[pl.ds(0, 3)], ys_s)
        drain(up2.at[pl.ds(0, 2)], u2a_ss)
        drain(up2.at[pl.ds(0, 2)], u2c_ss)
        drain(up2.at[pl.ds(0, 3)], u2b_ss)
        drain(xr.at[pl.ds(0, 15)], xs_s)
        drain(actr.at[pl.ds(0, 31)], as_s)
        drain(mr.at[pl.ds(0, 7)], ms_s)
        drain(rr, rs_s)
        drain(fr, fs_s.at[0])
        drain(fr.at[pl.ds(0, 3)], fs_s.at[1])


def local(stream, gain_first, up_first, down_first, gain_second, up_second, down_second):
    vmem = [
        ((32, 64), BF), ((2, 1, 32), F32), ((2, 32, 512), F32), ((2, 32, 512), F32),
        ((32, 512), BF), ((4, 32, 128), BF), ((2, 32, 512), BF),
        ((8, 8, 640), BF), ((8, 8, 512), BF), ((8, 8, 640), BF), ((8, 1152), BF), ((4, 8, 1152), BF),
        ((16, 32, 512), BF), ((4, 2, 32, 128), BF), ((8, 4, 2, 32, 128), BF),
        ((8, 256), BF), ((16, 8, 256), BF), ((2, 8, 128), BF), ((8, 8, 128), BF),
        ((8, 256), BF), ((32, 8, 256), BF), ((32, 64), BF), ((4, 32, 64), BF),
        ((32, 64), F32), ((32, 64), F32),
    ]
    dma = pltpu.SemaphoreType.DMA
    call = pl.pallas_call(
        kernel,
        out_shape=jax.ShapeDtypeStruct((32, 64), BF),
        in_specs=[pl.BlockSpec(memory_space=pl.ANY)] * 7,
        out_specs=pl.BlockSpec(memory_space=pltpu.VMEM),
        scratch_shapes=[pltpu.VMEM(*v) for v in vmem] + [dma((7,)), dma((2,)), dma((2,))] + [dma(())] * 29
        + [pltpu.SemaphoreType.REGULAR],
        compiler_params=pltpu.CompilerParams(collective_id=0, has_side_effects=True, vmem_limit_bytes=56535040),
    )
    out = call(
        stream.T, gain_first[None], up_first, down_first.T, gain_second[None], up_second, down_second.T
    )
    return out.T


def solution(mesh):
    in_specs = (P(None, "ra"), P("ra"), P("ra", "cb"), P("cb", "ra"), P("ra"), P("ra", "cb"), P("cb", "ra"))
    return jax.shard_map(local, mesh=mesh, in_specs=in_specs, out_specs=P(None, "ra"), check_vma=False)
```
